512 devices in a mesh: sp: 64 (over z, y), tp: 8 (over x, core).
Axes of the slice: x: 4, y: 8, z: 8, core: 2. Of those that a mesh axis runs over, the one named last changes fastest.
Arguments:
- queries: bfloat16 [32768, 2048], P('sp', 'tp'), may hold values from -6 to 6
- key_rows: bfloat16 [32768, 512], P('sp', 'tp'), may hold values from -6 to 6
- values: bfloat16 [32768, 512], P('sp', 'tp'), may hold values from -6 to 6
- sink_logit: float32 [32], P('tp'), may hold values from 4 to 10
- residual_in: bfloat16 [32768, 2048], P(('sp', 'tp')), may hold values from -6 to 6
- out_weight: bfloat16 [2048, 2048], P('tp'), may hold values from -0.125 to 0.125
- norm_gain: float32 [2048], replicated, may hold values from 0.1 to 1.9
- gate_weight: bfloat16 [2048, 5632], P('sp', 'tp'), may hold values from -0.125 to 0.125
- up_weight: bfloat16 [2048, 5632], P('sp', 'tp'), may hold values from -0.125 to 0.125
- down_weight: bfloat16 [5632, 2048], P('tp', 'sp'), may hold values from -0.078125 to 0.078125
Outputs:
- layer_out: bfloat16 [32768, 2048], P(('sp', 'tp'))
The draws below stay inside these ranges and needn't reach their ends.
All inputs are finite; a program needn't handle non-finite values.
Results may differ from the reference program's by a relative error of at most 0.013.
Values may be sent and summed in bfloat16 or wider, within the bound.
No kernel may reach another device: no remote copies, remote signals or barrier semaphores. Data moves between devices by JAX's collectives and lax.ppermute only.
A program may use at most 64 MiB of HBM per device.

```python
import jax
import jax.numpy as jnp
from jax import lax

D = 2048
HEADS = 32
KV_HEADS = 8
HEAD_DIM = 64
FF = 5632
WINDOW = 128
TOK_DEV = 512
TOKENS = 32768
N_TP = 8


def base_draw(key, columns):
    return jnp.clip(1.7 * jax.random.normal(key, (TOKENS, columns), jnp.float32), -6.0, 6.0)


def draw_queries(key, part):
    result = base_draw(jax.random.fold_in(key, 1), HEADS * HEAD_DIM)
    return result.astype(jnp.bfloat16)


def draw_key_rows(key, part):
    result = base_draw(jax.random.fold_in(key, 2), KV_HEADS * HEAD_DIM)
    return result.astype(jnp.bfloat16)


def level_of(stream_key, dims, split, least, high):
    loudness, own = 1.0, jax.random.fold_in(stream_key, 6)
    for dim, shards_of in split:
        steps = jnp.exp(jax.random.uniform(jax.random.fold_in(own, dim), (shards_of,), jnp.float32, least / len(split), high / len(split)))
        loudness = loudness * jnp.repeat(steps, dims[dim] // shards_of).reshape([-1 if axis == dim else 1 for axis in range(len(dims))])
    return loudness


def scatter_about(rng, dims, spread, limit, shards=(), kind=jnp.bfloat16):
    values = jax.random.normal(rng, dims, jnp.float32) * spread
    if len(shards) > 0:
        values = level_of(rng, dims, shards, -0.22, 0.18) * values
    return jnp.clip(values, min=-limit, max=limit).astype(kind)


def setup_inputs(seed: int = 0) -> dict:
    key_list = jax.random.split(jax.random.key(seed), 11)
    return {
        "queries": draw_queries(jax.random.fold_in(key_list[10], 71), 0),
        "key_rows": draw_key_rows(jax.random.fold_in(key_list[10], 71), 0),
        "values": scatter_about(key_list[2], (TOKENS, KV_HEADS * HEAD_DIM), 1.0, 6.0, ((0, 64), (1, 8))),
        "sink_logit": jnp.clip(4.0 + 6.0 * jax.random.uniform(key_list[3], (HEADS,), jnp.float32) ** level_of(key_list[3], (HEADS,), ((0, 8),), -0.2, 0.2), 4.0, 10.0),
        "residual_in": scatter_about(key_list[4], (TOKENS, D), 1.0, 6.0, ((0, 512),)),
        "out_weight": scatter_about(key_list[5], (HEADS * HEAD_DIM, D), (HEADS * HEAD_DIM) ** -0.5, 0.125, ((0, 8),)),
        "norm_gain": jnp.clip(1.0 + 0.18 * jax.random.normal(key_list[6], (D,), jnp.float32), 0.1, 1.9),
        "gate_weight": scatter_about(key_list[7], (D, FF), D ** -0.5, 0.125, ((0, 64), (1, 8))),
        "up_weight": scatter_about(key_list[8], (D, FF), D ** -0.5, 0.125, ((0, 64), (1, 8))),
        "down_weight": scatter_about(key_list[9], (FF, D), FF ** -0.5, 0.078125, ((0, 8), (1, 64))),
    }


def rms_scale(mixed_rows, norm_gain):
    inverse = lax.rsqrt(lax.optimization_barrier(jnp.mean(mixed_rows * mixed_rows, axis=-1, keepdims=True)) + 1e-06)
    return (mixed_rows * inverse * norm_gain).astype(jnp.bfloat16)

def rounded_sum(left, right, parts):
    columns = left.shape[1] // parts
    summed = jnp.zeros((left.shape[0], right.shape[1]), jnp.float32)
    for part_index in range(parts):
        partial_value = jnp.dot(left[:, part_index * columns:(part_index + 1) * columns], right[part_index * columns:(part_index + 1) * columns], preferred_element_type=jnp.float32)
        summed = summed + lax.optimization_barrier(partial_value.astype(jnp.bfloat16)).astype(jnp.float32)
    return summed

def reference(queries, key_rows, values, sink_logit, residual_in, out_weight, norm_gain, gate_weight, up_weight, down_weight):
    group_size = HEADS // KV_HEADS
    score_scale = HEAD_DIM ** (-0.5)
    block_count = TOKENS // WINDOW
    zero_rows = jnp.zeros((WINDOW, KV_HEADS * HEAD_DIM), jnp.bfloat16)
    key_padded = jnp.concatenate([zero_rows, key_rows, zero_rows], axis=0)
    value_padded = jnp.concatenate([zero_rows, values, zero_rows], axis=0)
    sink_grid = sink_logit.astype(jnp.float32).reshape(KV_HEADS, group_size)[:, :, None, None]

    def one_block(block_index):
        start_row = (block_index * WINDOW).astype(jnp.int32)
        query_block = lax.dynamic_slice_in_dim(queries, start_row, WINDOW, 0).astype(jnp.float32)
        query_block = query_block.reshape(WINDOW, KV_HEADS, group_size, HEAD_DIM)
        key_block = lax.dynamic_slice_in_dim(key_padded, start_row, 3 * WINDOW, 0).astype(jnp.float32)
        key_block = key_block.reshape(3 * WINDOW, KV_HEADS, HEAD_DIM)
        value_block = lax.dynamic_slice_in_dim(value_padded, start_row, 3 * WINDOW, 0).astype(jnp.float32)
        value_block = value_block.reshape(3 * WINDOW, KV_HEADS, HEAD_DIM)
        scores = jnp.einsum('qkgd,skd->kgqs', query_block, key_block) * score_scale
        query_pos = start_row + jnp.arange(WINDOW, dtype=jnp.int32)
        key_pos = start_row - WINDOW + jnp.arange(3 * WINDOW, dtype=jnp.int32)
        valid = (jnp.abs(query_pos[:, None] - key_pos[None, :]) <= WINDOW) & (key_pos >= 0)[None, :] & (key_pos < TOKENS)[None, :]
        scores = jnp.where(valid, scores, -1e+30)
        peak = jnp.maximum(lax.optimization_barrier(jnp.max(scores, axis=-1, keepdims=True)), sink_grid)
        weights_raw = jnp.exp(scores - peak)
        denom = lax.optimization_barrier(jnp.sum(weights_raw, axis=-1, keepdims=True)) + jnp.exp(sink_grid - peak)
        probs = lax.optimization_barrier((weights_raw / denom).astype(jnp.bfloat16)).astype(jnp.float32)
        output = jnp.einsum('kgqs,skd->qkgd', probs, value_block).astype(jnp.bfloat16)
        return output.reshape(WINDOW, HEADS * HEAD_DIM)
    attended = lax.map(one_block, jnp.arange(block_count, dtype=jnp.int32)).reshape(TOKENS, HEADS * HEAD_DIM)
    attn_sum = rounded_sum(attended, out_weight, N_TP)
    mixed_rows = residual_in.astype(jnp.float32) + attn_sum

    def feed_forward(mixed_block):
        normed = rms_scale(mixed_block, norm_gain)
        gate_pre = jnp.dot(normed, gate_weight, preferred_element_type=jnp.float32)
        up_pre = jnp.dot(normed, up_weight, preferred_element_type=jnp.float32)
        hidden = (jax.nn.silu(gate_pre) * up_pre).astype(jnp.bfloat16)
        ffn_sum = rounded_sum(hidden, down_weight, N_TP)
        return (mixed_block + ffn_sum).astype(jnp.bfloat16)
    blocked = mixed_rows.reshape(TOKENS // TOK_DEV, TOK_DEV, D)
    return lax.map(feed_forward, blocked).reshape(TOKENS, D)
```

```python
import functools

import jax
import jax.numpy as jnp
from jax import lax
from jax.experimental import pallas as pl
from jax.experimental.pallas import tpu as pltpu
from jax.sharding import PartitionSpec as P

HEAD_DIM = 64
WINDOW = 128
SIDE = 8
CORES = 2
LANES = 128


def device_index(sp, tp, tps):
    return sp * tps + tp


def line_groups(sps, tps, first):
    groups = []
    for tp in range(tps):
        along_y = (tp % CORES == 0) == first
        for fixed in range(sps // SIDE):
            line = [fixed * SIDE + k if along_y else k * SIDE + fixed for k in range(SIDE)]
            groups.append([device_index(sp, tp, tps) for sp in line])
    return groups


def x_groups(tps):
    return [[x * CORES + core for x in range(tps // CORES)] for core in range(CORES)]


def core_swap(tps):
    return [(i, i ^ 1) for i in range(tps)]


def ffn_kernel(core_ref, rows_ref, weights_ref, out_ref, held, hidden, sems, *, hid):
    full = hid // LANES
    rest = hid - full * LANES
    gated = 2 * hid
    parts = [(2 * LANES * j, 2 * LANES) for j in range(full)] + [(2 * LANES * full, 2 * rest)]
    parts.append((gated, hid))
    core = core_ref[0]

    def copies(part, swapped):
        at, size = parts[part]
        return [
            pltpu.make_async_copy(
                weights_ref.at[:, i, :, pl.ds(at, size)]
                if swapped
                else weights_ref.at[i, :, :, pl.ds(at, size)],
                held.at[i, :, :, pl.ds(at, size)],
                sems.at[part],
            )
            for i in range(SIDE)
        ]

    for swapped in (False, True):

        @pl.when(core == int(swapped))
        def _():
            for part in range(len(parts)):
                for copy in copies(part, swapped):
                    copy.start()

    depth = rows_ref.shape[1]
    for part in range(full + 1):
        at, size = parts[part]
        for copy in copies(part, False):
            copy.wait()
        tile = held[:, :, :, at : at + size].reshape(depth, size)
        both = jnp.dot(rows_ref[...], tile, preferred_element_type=jnp.float32)
        gate, up = both[:, : size // 2], both[:, size // 2 :]
        hidden[:, at // 2 : at // 2 + size // 2] = (gate / (1.0 + jnp.exp(-gate)) * up).astype(
            hidden.dtype
        )
    for copy in copies(full + 1, False):
        copy.wait()
    for i in range(SIDE):
        tile = held[i, :, :, gated : gated + hid].reshape(-1, hid)
        width = tile.shape[0]
        out_ref[:, i * width : (i + 1) * width] = lax.dot_general(
            hidden[...], tile, (((1,), (1,)), ((), ())), preferred_element_type=jnp.float32
        ).astype(out_ref.dtype)


def feed_forward(rows, weights, core, out_dtype):
    count, depth = rows.shape
    piece, width = weights.shape[2:]
    hid = width // 3
    parts = hid // LANES + 2
    return pl.pallas_call(
        functools.partial(ffn_kernel, hid=hid),
        out_shape=jax.ShapeDtypeStruct((count, depth), out_dtype),
        in_specs=[
            pl.BlockSpec(memory_space=pltpu.SMEM),
            pl.BlockSpec(memory_space=pltpu.VMEM),
            pl.BlockSpec(memory_space=pl.ANY),
        ],
        out_specs=pl.BlockSpec(memory_space=pltpu.VMEM),
        scratch_shapes=[
            pltpu.VMEM((SIDE, SIDE, piece, width), jnp.bfloat16),
            pltpu.VMEM((count, hid), jnp.bfloat16),
            pltpu.SemaphoreType.DMA((parts,)),
        ],
        cost_estimate=pl.CostEstimate(
            flops=2 * count * depth * width,
            bytes_accessed=2 * weights.size + 4 * rows.size,
            transcendentals=count * hid,
        ),
        compiler_params=pltpu.CompilerParams(vmem_limit_bytes=40 * 1024 * 1024),
        name="ffn",
    )(core, rows, weights)


def with_halo(block, axis, width):
    count = lax.axis_size(axis)
    forward = [(i, i + 1) for i in range(count - 1)]
    backward = [(target, source) for source, target in forward]
    low = lax.ppermute(block[-width:], axis, forward)
    high = lax.ppermute(block[:width], axis, backward)
    return jnp.concatenate([low, block, high], axis=0)


def attend_window(queries, padded, offset, total_rows, sink_logit):
    rows_here = queries.shape[0]
    block_count = rows_here // WINDOW
    heads_here = queries.shape[1] // HEAD_DIM
    kv_here = padded.shape[1] // (2 * HEAD_DIM)
    group_size = heads_here // kv_here
    blocks = padded.reshape(block_count + 2, WINDOW, padded.shape[1])
    banded = jnp.concatenate([blocks[:-2], blocks[1:-1], blocks[2:]], axis=1)
    key_band = banded[:, :, : kv_here * HEAD_DIM].reshape(
        block_count, 3 * WINDOW, kv_here, HEAD_DIM
    )
    value_band = banded[:, :, kv_here * HEAD_DIM :].reshape(
        block_count, 3 * WINDOW, kv_here, HEAD_DIM
    )
    grouped = queries.reshape(block_count, WINDOW, kv_here, group_size, HEAD_DIM)
    scores = jnp.einsum(
        "nqkgd,nskd->nkgqs", grouped, key_band, preferred_element_type=jnp.float32
    ) * HEAD_DIM ** (-0.5)
    block_start = offset + jnp.arange(block_count, dtype=jnp.int32)[:, None] * WINDOW
    query_pos = block_start + jnp.arange(WINDOW, dtype=jnp.int32)[None, :]
    key_pos = block_start - WINDOW + jnp.arange(3 * WINDOW, dtype=jnp.int32)[None, :]
    valid = jnp.abs(query_pos[:, :, None] - key_pos[:, None, :]) <= WINDOW
    valid = valid & ((key_pos >= 0) & (key_pos < total_rows))[:, None, :]
    scores = jnp.where(valid[:, None, None], scores, -1e30)
    sink_grid = sink_logit.reshape(kv_here, group_size)[None, :, :, None, None]
    peak = jnp.maximum(jnp.max(scores, axis=-1, keepdims=True), sink_grid)
    weights_raw = jnp.exp(scores - peak)
    denom = jnp.sum(weights_raw, axis=-1, keepdims=True) + jnp.exp(sink_grid - peak)
    probs = (weights_raw / denom).astype(jnp.bfloat16)
    output = jnp.einsum("nkgqs,nskd->nqkgd", probs, value_band, preferred_element_type=jnp.float32)
    return output.astype(jnp.bfloat16).reshape(rows_here, heads_here * HEAD_DIM)


def rms_scale(mixed_rows, norm_gain):
    inverse = lax.rsqrt(jnp.mean(mixed_rows * mixed_rows, axis=-1, keepdims=True) + 1e-06)
    return (mixed_rows * inverse * norm_gain).astype(jnp.bfloat16)


def joined_weights(gate_weight, up_weight, down_weight):
    hid = gate_weight.shape[1]
    pieces = []
    for at in range(0, hid, LANES):
        pieces += [gate_weight[:, at : at + LANES], up_weight[:, at : at + LANES]]
    return jnp.concatenate(pieces + [down_weight.T], axis=1)


def shards(
    queries,
    key_rows,
    values,
    sink_logit,
    residual_in,
    out_weight,
    norm_gain,
    gate_weight,
    up_weight,
    down_weight,
):
    rows_here, depth = queries.shape[0], residual_in.shape[1]
    sps, tps = lax.axis_size("sp"), lax.axis_size("tp")
    xs = tps // CORES
    own = rows_here // tps
    core = lax.axis_index("tp") % CORES
    both_axes = ("sp", "tp")

    mine = joined_weights(gate_weight, up_weight, down_weight)
    line = lax.all_to_all(
        jnp.broadcast_to(mine[None], (SIDE, *mine.shape)),
        both_axes,
        0,
        0,
        tiled=True,
        axis_index_groups=line_groups(sps, tps, True),
    )
    line, queries, key_rows, values = lax.optimization_barrier((line, queries, key_rows, values))
    weights = lax.all_gather(
        line, both_axes, axis=0, tiled=False, axis_index_groups=line_groups(sps, tps, False)
    )

    joined = jnp.concatenate([key_rows, values], axis=1)
    padded = with_halo(joined, "sp", WINDOW)
    offset = lax.axis_index("sp") * rows_here
    attended = attend_window(queries, padded, offset, rows_here * sps, sink_logit)

    by_core = attended.reshape(xs, CORES, own, attended.shape[1])
    even, odd = by_core[:, 0], by_core[:, 1]
    for_me = jnp.where(core == 0, even, odd).reshape(xs * own, -1)
    for_mate = jnp.where(core == 0, odd, even).reshape(xs * own, -1)

    def swap(array):
        return lax.ppermute(array, "tp", core_swap(tps))

    def summed(partial):
        pieces = lax.all_to_all(
            partial.reshape(xs, own, depth), "tp", 0, 0, tiled=True, axis_index_groups=x_groups(tps)
        )
        return jnp.sum(pieces.astype(jnp.float32), axis=0)

    mate_part = swap(
        jnp.dot(for_mate, out_weight, preferred_element_type=jnp.float32).astype(jnp.bfloat16)
    )
    my_part = jnp.dot(for_me, out_weight, preferred_element_type=jnp.float32)
    attn_sum = summed((my_part + mate_part.astype(jnp.float32)).astype(jnp.bfloat16))
    mixed_rows = residual_in.astype(jnp.float32) + attn_sum

    normed = rms_scale(mixed_rows, norm_gain)
    my_rows = lax.all_to_all(
        jnp.broadcast_to(normed[None], (xs, own, depth)),
        "tp",
        0,
        0,
        tiled=True,
        axis_index_groups=x_groups(tps),
    ).reshape(xs * own, depth)
    mate_rows = swap(my_rows)
    core_scalar = core.astype(jnp.int32).reshape(1)
    mate_out = feed_forward(mate_rows, weights, core_scalar, jnp.bfloat16)
    mate_sum = swap(mate_out)
    my_out = feed_forward(my_rows, weights, core_scalar, jnp.float32)
    ffn_sum = summed((my_out + mate_sum.astype(jnp.float32)).astype(jnp.bfloat16))
    return (mixed_rows + ffn_sum).astype(jnp.bfloat16)


def solution(mesh):
    return jax.shard_map(
        shards,
        mesh=mesh,
        in_specs=(
            P("sp", "tp"),
            P("sp", "tp"),
            P("sp", "tp"),
            P("tp"),
            P(("sp", "tp"), None),
            P("tp", None),
            P(),
            P("sp", "tp"),
            P("sp", "tp"),
            P("tp", "sp"),
        ),
        out_specs=P(("sp", "tp"), None),
        check_vma=False,
    )
```

```python
import functools

import jax
import jax.numpy as jnp
from jax import lax
from jax.experimental import pallas as pl
from jax.experimental.pallas import tpu as pltpu
from jax.sharding import PartitionSpec as P

HEAD_DIM = 64
WINDOW = 128
SIDE = 8
CORES = 2
FIRST_VMEM = 40 * 1024 * 1024


def device_index(sp, tp, tps):
    return sp * tps + tp


def line_groups(sps, tps, first):
    groups = []
    for tp in range(tps):
        along_y = (tp % CORES == 0) == first
        for fixed in range(sps // SIDE):
            line = [fixed * SIDE + k if along_y else k * SIDE + fixed for k in range(SIDE)]
            groups.append([device_index(sp, tp, tps) for sp in line])
    return groups


def x_groups(tps):
    return [[x * CORES + core for x in range(tps // CORES)] for core in range(CORES)]


def core_swap(tps):
    return [(i, i ^ 1) for i in range(tps)]


def joined_kernel(gate_ref, up_ref, down_ref, out_ref):
    mine = jnp.concatenate([gate_ref[...], up_ref[...], down_ref[...]], axis=1)
    for i in range(out_ref.shape[0]):
        out_ref[i] = mine


def joined_weights(gate_weight, up_weight, down_weight):
    piece, hid = gate_weight.shape
    return pl.pallas_call(
        joined_kernel,
        out_shape=jax.ShapeDtypeStruct((SIDE, piece, 3 * hid), gate_weight.dtype),
        in_specs=[pl.BlockSpec(memory_space=pltpu.VMEM)] * 3,
        out_specs=pl.BlockSpec(memory_space=pltpu.VMEM),
        compiler_params=pltpu.CompilerParams(vmem_limit_bytes=4 * 1024 * 1024),
        name="joined",
    )(gate_weight, up_weight, down_weight.T)


def gated_product(both, hid):
    gate, up = both[:, :hid], both[:, hid:]
    return (gate / (1.0 + jnp.exp(-gate)) * up).astype(jnp.bfloat16)


def down_product(hidden, down):
    return lax.dot_general(hidden, down, (((1,), (1,)), ((), ())), preferred_element_type=jnp.float32)


def first_kernel(core_ref, rows_ref, weights_ref, out_ref, held, total, sems, *, hid):
    piece = held.shape[2]
    per = 2
    span = per * SIDE * piece
    core = core_ref[0]

    def copy(i, swapped):
        source = weights_ref.at[:, i] if swapped else weights_ref.at[i]
        return pltpu.make_async_copy(source, held.at[i], sems.at[i])

    for swapped in (False, True):

        @pl.when(core == int(swapped))
        def _():
            for i in range(SIDE):
                copy(i, swapped).start()

    both = None
    for step in range(SIDE // per):
        for i in range(step * per, (step + 1) * per):
            copy(i, False).wait()
        tile = held[step * per : (step + 1) * per, :, :, : 2 * hid].reshape(span, 2 * hid)
        part = jnp.dot(
            rows_ref[:, step * span : (step + 1) * span], tile, preferred_element_type=jnp.float32
        )
        if step == 0:
            total[...] = part
        elif step < SIDE // per - 1:
            total[...] += part
        else:
            both = total[...] + part
    down = held[:, :, :, 2 * hid :].reshape(-1, hid)
    out_ref[...] = down_product(gated_product(both, hid), down).astype(out_ref.dtype)


def second_kernel(rows_ref, held, out_ref, *, hid):
    tile = held[:, :, :, : 2 * hid].reshape(-1, 2 * hid)
    both = jnp.dot(rows_ref[...], tile, preferred_element_type=jnp.float32)
    down = held[:, :, :, 2 * hid :].reshape(-1, hid)
    out_ref[...] = down_product(gated_product(both, hid), down).astype(out_ref.dtype)


def ffn_cost(rows, width):
    count, depth = rows.shape
    return pl.CostEstimate(
        flops=2 * count * depth * width,
        bytes_accessed=2 * depth * width + 4 * rows.size,
        transcendentals=count * width // 3,
    )


def feed_forward_first(rows, weights, core):
    count, depth = rows.shape
    width = weights.shape[3]
    vmem = pl.BlockSpec(memory_space=pltpu.VMEM)
    return pl.pallas_call(
        functools.partial(first_kernel, hid=width // 3),
        out_shape=(
            jax.ShapeDtypeStruct((count, depth), jnp.bfloat16),
            jax.ShapeDtypeStruct(weights.shape, weights.dtype),
        ),
        in_specs=[
            pl.BlockSpec(memory_space=pltpu.SMEM),
            vmem,
            pl.BlockSpec(memory_space=pl.ANY),
        ],
        out_specs=(vmem, vmem),
        scratch_shapes=[
            pltpu.VMEM((count, 2 * width // 3), jnp.float32),
            pltpu.SemaphoreType.DMA((SIDE,)),
        ],
        cost_estimate=ffn_cost(rows, width),
        compiler_params=pltpu.CompilerParams(vmem_limit_bytes=FIRST_VMEM),
        name="ffn_first",
    )(core, rows, weights)


def feed_forward_second(rows, held):
    width = held.shape[3]
    vmem = pl.BlockSpec(memory_space=pltpu.VMEM)
    return pl.pallas_call(
        functools.partial(second_kernel, hid=width // 3),
        out_shape=jax.ShapeDtypeStruct(rows.shape, jnp.float32),
        in_specs=[vmem, vmem],
        out_specs=vmem,
        cost_estimate=ffn_cost(rows, width),
        compiler_params=pltpu.CompilerParams(vmem_limit_bytes=24 * 1024 * 1024),
        name="ffn_second",
    )(rows, held)


def with_halo(block, axis, width):
    count = lax.axis_size(axis)
    forward = [(i, i + 1) for i in range(count - 1)]
    backward = [(target, source) for source, target in forward]
    low = lax.ppermute(block[-width:], axis, forward)
    high = lax.ppermute(block[:width], axis, backward)
    return jnp.concatenate([low, block, high], axis=0)


def attend_window(queries, padded, offset, total_rows, sink_logit):
    rows_here = queries.shape[0]
    block_count = rows_here // WINDOW
    heads_here = queries.shape[1] // HEAD_DIM
    kv_here = padded.shape[1] // (2 * HEAD_DIM)
    group_size = heads_here // kv_here
    blocks = padded.reshape(block_count + 2, WINDOW, padded.shape[1])
    banded = jnp.concatenate([blocks[:-2], blocks[1:-1], blocks[2:]], axis=1)
    key_band = banded[:, :, : kv_here * HEAD_DIM].reshape(
        block_count, 3 * WINDOW, kv_here, HEAD_DIM
    )
    value_band = banded[:, :, kv_here * HEAD_DIM :].reshape(
        block_count, 3 * WINDOW, kv_here, HEAD_DIM
    )
    grouped = queries.reshape(block_count, WINDOW, kv_here, group_size, HEAD_DIM)
    scores = jnp.einsum(
        "nqkgd,nskd->nkgqs", grouped, key_band, preferred_element_type=jnp.float32
    ) * HEAD_DIM ** (-0.5)
    block_start = offset + jnp.arange(block_count, dtype=jnp.int32)[:, None] * WINDOW
    query_pos = block_start + jnp.arange(WINDOW, dtype=jnp.int32)[None, :]
    key_pos = block_start - WINDOW + jnp.arange(3 * WINDOW, dtype=jnp.int32)[None, :]
    valid = jnp.abs(query_pos[:, :, None] - key_pos[:, None, :]) <= WINDOW
    valid = valid & ((key_pos >= 0) & (key_pos < total_rows))[:, None, :]
    scores = jnp.where(valid[:, None, None], scores, -1e30)
    sink_grid = sink_logit.reshape(kv_here, group_size)[None, :, :, None, None]
    peak = jnp.maximum(jnp.max(scores, axis=-1, keepdims=True), sink_grid)
    weights_raw = jnp.exp(scores - peak)
    denom = jnp.sum(weights_raw, axis=-1, keepdims=True) + jnp.exp(sink_grid - peak)
    probs = (weights_raw / denom).astype(jnp.bfloat16)
    output = jnp.einsum("nkgqs,nskd->nqkgd", probs, value_band, preferred_element_type=jnp.float32)
    return output.astype(jnp.bfloat16).reshape(rows_here, heads_here * HEAD_DIM)


def rms_scale(mixed_rows, norm_gain):
    inverse = lax.rsqrt(jnp.mean(mixed_rows * mixed_rows, axis=-1, keepdims=True) + 1e-06)
    return (mixed_rows * inverse * norm_gain).astype(jnp.bfloat16)


def shards(
    queries,
    key_rows,
    values,
    sink_logit,
    residual_in,
    out_weight,
    norm_gain,
    gate_weight,
    up_weight,
    down_weight,
):
    rows_here, depth = queries.shape[0], residual_in.shape[1]
    sps, tps = lax.axis_size("sp"), lax.axis_size("tp")
    xs = tps // CORES
    own = rows_here // tps
    core = lax.axis_index("tp") % CORES
    both_axes = ("sp", "tp")

    mine = joined_weights(gate_weight, up_weight, down_weight)
    line = lax.all_to_all(
        mine,
        both_axes,
        0,
        0,
        tiled=True,
        axis_index_groups=line_groups(sps, tps, True),
    )
    line, queries, key_rows, values = lax.optimization_barrier((line, queries, key_rows, values))
    weights = lax.all_gather(
        line, both_axes, axis=0, tiled=False, axis_index_groups=line_groups(sps, tps, False)
    )

    joined = jnp.concatenate([key_rows, values], axis=1)
    padded = with_halo(joined, "sp", WINDOW)
    offset = lax.axis_index("sp") * rows_here
    attended = attend_window(queries, padded, offset, rows_here * sps, sink_logit)

    by_core = attended.reshape(xs, CORES, own, attended.shape[1])
    even, odd = by_core[:, 0], by_core[:, 1]
    for_me = jnp.where(core == 0, even, odd).reshape(xs * own, -1)
    for_mate = jnp.where(core == 0, odd, even).reshape(xs * own, -1)

    def swap(array):
        return lax.ppermute(array, "tp", core_swap(tps))

    def summed(partial):
        pieces = lax.all_to_all(
            partial.reshape(xs, own, depth), "tp", 0, 0, tiled=True, axis_index_groups=x_groups(tps)
        )
        return jnp.sum(pieces.astype(jnp.float32), axis=0)

    mate_part = swap(
        jnp.dot(for_mate, out_weight, preferred_element_type=jnp.float32).astype(jnp.bfloat16)
    )
    my_part = jnp.dot(for_me, out_weight, preferred_element_type=jnp.float32)
    attn_sum = summed((my_part + mate_part.astype(jnp.float32)).astype(jnp.bfloat16))
    mixed_rows = residual_in.astype(jnp.float32) + attn_sum

    normed = rms_scale(mixed_rows, norm_gain)
    my_rows = lax.all_to_all(
        jnp.broadcast_to(normed[None], (xs, own, depth)),
        "tp",
        0,
        0,
        tiled=True,
        axis_index_groups=x_groups(tps),
    ).reshape(xs * own, depth)
    mate_rows = swap(my_rows)
    core_scalar = core.astype(jnp.int32).reshape(1)
    mate_out, held = feed_forward_first(mate_rows, weights, core_scalar)
    mate_sum = swap(mate_out)
    my_out = feed_forward_second(my_rows, held)
    ffn_sum = summed((my_out + mate_sum.astype(jnp.float32)).astype(jnp.bfloat16))
    return (mixed_rows + ffn_sum).astype(jnp.bfloat16)


def solution(mesh):
    return jax.shard_map(
        shards,
        mesh=mesh,
        in_specs=(
            P("sp", "tp"),
            P("sp", "tp"),
            P("sp", "tp"),
            P("tp"),
            P(("sp", "tp"), None),
            P("tp", None),
            P(),
            P("sp", "tp"),
            P("sp", "tp"),
            P("tp", "sp"),
        ),
        out_specs=P(("sp", "tp"), None),
        check_vma=False,
    )
```

```python
import functools

import jax
import jax.numpy as jnp
from jax import lax
from jax.experimental import pallas as pl
from jax.experimental.pallas import tpu as pltpu
from jax.sharding import PartitionSpec as P

HEAD_DIM = 64
WINDOW = 128
SIDE = 8
CORES = 2
FIRST_VMEM = 40 * 1024 * 1024


def device_index(sp, tp, tps):
    return sp * tps + tp


def line_groups(sps, tps, first):
    groups = []
    for tp in range(tps):
        along_y = (tp % CORES == 0) == first
        for fixed in range(sps // SIDE):
            line = [fixed * SIDE + k if along_y else k * SIDE + fixed for k in range(SIDE)]
            groups.append([device_index(sp, tp, tps) for sp in line])
    return groups


def x_groups(tps):
    return [[x * CORES + core for x in range(tps // CORES)] for core in range(CORES)]


def core_swap(tps):
    return [(i, i ^ 1) for i in range(tps)]


def gated_product(both, hid):
    gate, up = both[:, :hid], both[:, hid:]
    return (gate / (1.0 + jnp.exp(-gate)) * up).astype(jnp.bfloat16)


def down_product(hidden, down):
    return lax.dot_general(hidden, down, (((1,), (1,)), ((), ())), preferred_element_type=jnp.float32)


def first_kernel(core_ref, rows_ref, weights_ref, out_ref, held, total, sems, *, hid):
    piece = held.shape[2]
    per = 2
    span = per * SIDE * piece
    core = core_ref[0]

    def copy(i, swapped):
        source = weights_ref.at[:, i] if swapped else weights_ref.at[i]
        return pltpu.make_async_copy(source, held.at[i], sems.at[i])

    for swapped in (False, True):

        @pl.when(core == int(swapped))
        def _():
            for i in range(SIDE):
                copy(i, swapped).start()

    both = None
    for step in range(SIDE // per):
        for i in range(step * per, (step + 1) * per):
            copy(i, False).wait()
        tile = held[step * per : (step + 1) * per, :, :, : 2 * hid].reshape(span, 2 * hid)
        part = jnp.dot(
            rows_ref[:, step * span : (step + 1) * span], tile, preferred_element_type=jnp.float32
        )
        if step == 0:
            total[...] = part
        elif step < SIDE // per - 1:
            total[...] += part
        else:
            both = total[...] + part
    down = held[:, :, :, 2 * hid :].reshape(-1, hid)
    out_ref[...] = down_product(gated_product(both, hid), down).astype(out_ref.dtype)


def second_kernel(rows_ref, held, out_ref, *, hid):
    tile = held[:, :, :, : 2 * hid].reshape(-1, 2 * hid)
    both = jnp.dot(rows_ref[...], tile, preferred_element_type=jnp.float32)
    down = held[:, :, :, 2 * hid :].reshape(-1, hid)
    out_ref[...] = down_product(gated_product(both, hid), down).astype(out_ref.dtype)


def ffn_cost(rows, width):
    count, depth = rows.shape
    return pl.CostEstimate(
        flops=2 * count * depth * width,
        bytes_accessed=2 * depth * width + 4 * rows.size,
        transcendentals=count * width // 3,
    )


def feed_forward_first(rows, weights, core):
    count, depth = rows.shape
    width = weights.shape[3]
    vmem = pl.BlockSpec(memory_space=pltpu.VMEM)
    return pl.pallas_call(
        functools.partial(first_kernel, hid=width // 3),
        out_shape=(
            jax.ShapeDtypeStruct((count, depth), jnp.bfloat16),
            jax.ShapeDtypeStruct(weights.shape, weights.dtype),
        ),
        in_specs=[
            pl.BlockSpec(memory_space=pltpu.SMEM),
            vmem,
            pl.BlockSpec(memory_space=pl.ANY),
        ],
        out_specs=(vmem, vmem),
        scratch_shapes=[
            pltpu.VMEM((count, 2 * width // 3), jnp.float32),
            pltpu.SemaphoreType.DMA((SIDE,)),
        ],
        cost_estimate=ffn_cost(rows, width),
        compiler_params=pltpu.CompilerParams(vmem_limit_bytes=FIRST_VMEM),
        name="ffn_first",
    )(core, rows, weights)


def feed_forward_second(rows, held):
    width = held.shape[3]
    vmem = pl.BlockSpec(memory_space=pltpu.VMEM)
    return pl.pallas_call(
        functools.partial(second_kernel, hid=width // 3),
        out_shape=jax.ShapeDtypeStruct(rows.shape, jnp.float32),
        in_specs=[vmem, vmem],
        out_specs=vmem,
        cost_estimate=ffn_cost(rows, width),
        compiler_params=pltpu.CompilerParams(vmem_limit_bytes=24 * 1024 * 1024),
        name="ffn_second",
    )(rows, held)


def halo_sides(block, axis, width):
    count = lax.axis_size(axis)
    forward = [(i, i + 1) for i in range(count - 1)]
    backward = [(target, source) for source, target in forward]
    low = lax.ppermute(block[:, -width:], axis, forward)
    high = lax.ppermute(block[:, :width], axis, backward)
    return low, high


def attention_kernel(
    place_ref, sink_ref, query_ref, low_ref, mid_ref, high_ref, proj_ref, mate_ref, mine_ref, padded, attended
):
    rows = query_ref.shape[0]
    heads = query_ref.shape[1] // HEAD_DIM
    piece = WINDOW // CORES
    core, start, total = place_ref[0], place_ref[1], place_ref[2]
    padded[:, :WINDOW] = low_ref[...]
    padded[:, WINDOW : WINDOW + rows] = mid_ref[...]
    padded[:, WINDOW + rows :] = high_ref[...]
    query_at = lax.broadcasted_iota(jnp.int32, (WINDOW, 3 * WINDOW), 0)
    key_at = lax.broadcasted_iota(jnp.int32, (WINDOW, 3 * WINDOW), 1)
    near = (key_at >= query_at) & (key_at <= query_at + 2 * WINDOW)
    for block in range(rows // WINDOW):
        at = block * WINDOW
        position = key_at + (start + at - WINDOW)
        valid = near & (position >= 0) & (position < total)
        keys = padded[:HEAD_DIM, at : at + 3 * WINDOW]
        values = padded[HEAD_DIM:, at : at + 3 * WINDOW]
        for head in range(heads):
            lanes = slice(head * HEAD_DIM, (head + 1) * HEAD_DIM)
            scores = jnp.dot(
                query_ref[at : at + WINDOW, lanes], keys, preferred_element_type=jnp.float32
            ) * HEAD_DIM ** (-0.5)
            scores = jnp.where(valid, scores, -1e30)
            sink = sink_ref[head]
            peak = jnp.maximum(jnp.max(scores, axis=1, keepdims=True), sink)
            raw = jnp.exp(scores - peak)
            denom = jnp.sum(raw, axis=1, keepdims=True) + jnp.exp(sink - peak)
            probs = (raw * (1.0 / denom)).astype(jnp.bfloat16)
            attended[at : at + WINDOW, lanes] = lax.dot_general(
                probs, values, (((1,), (1,)), ((), ())), preferred_element_type=jnp.float32
            ).astype(jnp.bfloat16)
    for target, which in ((mate_ref, 1 - core), (mine_ref, core)):
        picked = jnp.concatenate(
            [
                attended[pl.ds(pl.multiple_of(at + which * piece, piece), piece), :]
                for at in range(0, rows, WINDOW)
            ],
            axis=0,
        )
        target[...] = jnp.dot(picked, proj_ref[...], preferred_element_type=jnp.float32).astype(
            target.dtype
        )


def attend_and_project(queries, sides, middle, sink_logit, out_weight, place):
    rows, columns = queries.shape
    depth = out_weight.shape[1]
    low, high = sides
    vmem = pl.BlockSpec(memory_space=pltpu.VMEM)
    smem = pl.BlockSpec(memory_space=pltpu.SMEM)
    half = rows // CORES
    return pl.pallas_call(
        attention_kernel,
        out_shape=(
            jax.ShapeDtypeStruct((half, depth), jnp.bfloat16),
            jax.ShapeDtypeStruct((half, depth), jnp.float32),
        ),
        in_specs=[smem, smem, vmem, vmem, vmem, vmem, vmem],
        out_specs=(vmem, vmem),
        scratch_shapes=[
            pltpu.VMEM((2 * HEAD_DIM, rows + 2 * WINDOW), jnp.bfloat16),
            pltpu.VMEM((rows, columns), jnp.bfloat16),
        ],
        cost_estimate=pl.CostEstimate(
            flops=2 * rows * columns * (6 * WINDOW + depth),
            bytes_accessed=8 * half * depth,
            transcendentals=3 * WINDOW * rows * columns // HEAD_DIM,
        ),
        compiler_params=pltpu.CompilerParams(vmem_limit_bytes=16 * 1024 * 1024),
        name="attend",
    )(place, sink_logit, queries, low, middle, high, out_weight)


def rms_scale(mixed_rows, norm_gain):
    inverse = lax.rsqrt(jnp.mean(mixed_rows * mixed_rows, axis=-1, keepdims=True) + 1e-06)
    return (mixed_rows * inverse * norm_gain).astype(jnp.bfloat16)


def shards(
    queries,
    key_rows,
    values,
    sink_logit,
    residual_in,
    out_weight,
    norm_gain,
    gate_weight,
    up_weight,
    down_weight,
):
    rows_here, depth = queries.shape[0], residual_in.shape[1]
    sps, tps = lax.axis_size("sp"), lax.axis_size("tp")
    xs = tps // CORES
    own = rows_here // tps
    core = lax.axis_index("tp") % CORES
    both_axes = ("sp", "tp")

    mine = jnp.concatenate([gate_weight, up_weight, down_weight.T], axis=1)
    line = lax.all_to_all(
        jnp.broadcast_to(mine[None], (SIDE, *mine.shape)),
        both_axes,
        0,
        0,
        tiled=True,
        axis_index_groups=line_groups(sps, tps, True),
    )
    line, queries, key_rows, values = lax.optimization_barrier((line, queries, key_rows, values))
    weights = lax.all_gather(
        line, both_axes, axis=0, tiled=False, axis_index_groups=line_groups(sps, tps, False)
    )

    middle = jnp.concatenate([key_rows.T, values.T], axis=0)
    sides = halo_sides(middle, "sp", WINDOW)
    place = jnp.stack([core, lax.axis_index("sp") * rows_here, jnp.int32(rows_here * sps)]).astype(
        jnp.int32
    )

    def swap(array):
        return lax.ppermute(array, "tp", core_swap(tps))

    def summed(partial):
        pieces = lax.all_to_all(
            partial.reshape(xs, own, depth), "tp", 0, 0, tiled=True, axis_index_groups=x_groups(tps)
        )
        return jnp.sum(pieces.astype(jnp.float32), axis=0)

    mate_part, my_part = attend_and_project(
        queries, sides, middle, sink_logit, out_weight, place
    )
    attn_sum = summed((my_part + swap(mate_part).astype(jnp.float32)).astype(jnp.bfloat16))
    mixed_rows = residual_in.astype(jnp.float32) + attn_sum

    normed = rms_scale(mixed_rows, norm_gain)
    my_rows = lax.all_to_all(
        jnp.broadcast_to(normed[None], (xs, own, depth)),
        "tp",
        0,
        0,
        tiled=True,
        axis_index_groups=x_groups(tps),
    ).reshape(xs * own, depth)
    mate_rows = swap(my_rows)
    core_scalar = core.astype(jnp.int32).reshape(1)
    mate_out, held = feed_forward_first(mate_rows, weights, core_scalar)
    mate_sum = swap(mate_out)
    my_out = feed_forward_second(my_rows, held)
    ffn_sum = summed((my_out + mate_sum.astype(jnp.float32)).astype(jnp.bfloat16))
    return (mixed_rows + ffn_sum).astype(jnp.bfloat16)


def solution(mesh):
    return jax.shard_map(
        shards,
        mesh=mesh,
        in_specs=(
            P("sp", "tp"),
            P("sp", "tp"),
            P("sp", "tp"),
            P("tp"),
            P(("sp", "tp"), None),
            P("tp", None),
            P(),
            P("sp", "tp"),
            P("sp", "tp"),
            P("tp", "sp"),
        ),
        out_specs=P(("sp", "tp"), None),
        check_vma=False,
    )
```

```python
import functools

import jax
import jax.numpy as jnp
from jax import lax
from jax.experimental import pallas as pl
from jax.experimental.pallas import tpu as pltpu
from jax.sharding import PartitionSpec as P

HEAD_DIM = 64
WINDOW = 128
SIDE = 8
CORES = 2
FIRST_VMEM = 40 * 1024 * 1024


def device_index(sp, tp, tps):
    return sp * tps + tp


def line_groups(sps, tps, first):
    groups = []
    for tp in range(tps):
        along_y = (tp % CORES == 0) == first
        for fixed in range(sps // SIDE):
            line = [fixed * SIDE + k if along_y else k * SIDE + fixed for k in range(SIDE)]
            groups.append([device_index(sp, tp, tps) for sp in line])
    return groups


def x_groups(tps):
    return [[x * CORES + core for x in range(tps // CORES)] for core in range(CORES)]


def core_swap(tps):
    return [(i, i ^ 1) for i in range(tps)]


def gated_product(both, hid):
    gate, up = both[:, :hid], both[:, hid:]
    return (gate / (1.0 + jnp.exp(-gate)) * up).astype(jnp.bfloat16)


def down_product(hidden, down):
    return lax.dot_general(hidden, down, (((1,), (1,)), ((), ())), preferred_element_type=jnp.float32)


def first_kernel(core_ref, rows_ref, weights_ref, out_ref, held, total, sems, *, hid):
    piece = held.shape[2]
    per = 2
    span = per * SIDE * piece
    core = core_ref[0]

    def copy(i, swapped, part):
        columns = (pl.ds(0, 2 * hid), pl.ds(2 * hid, hid))[part]
        source = weights_ref.at[:, i, :, columns] if swapped else weights_ref.at[i, :, :, columns]
        return pltpu.make_async_copy(source, held.at[i, :, :, columns], sems.at[part, i])

    for swapped in (False, True):

        @pl.when(core == int(swapped))
        def _():
            for part in range(2):
                for i in range(SIDE):
                    copy(i, swapped, part).start()

    both = None
    for step in range(SIDE // per):
        for i in range(step * per, (step + 1) * per):
            copy(i, False, 0).wait()
        tile = held[step * per : (step + 1) * per, :, :, : 2 * hid].reshape(span, 2 * hid)
        part = jnp.dot(
            rows_ref[:, step * span : (step + 1) * span], tile, preferred_element_type=jnp.float32
        )
        if step == 0:
            total[...] = part
        elif step < SIDE // per - 1:
            total[...] += part
        else:
            both = total[...] + part
    hidden = gated_product(both, hid)
    for i in range(SIDE):
        copy(i, False, 1).wait()
    down = held[:, :, :, 2 * hid :].reshape(-1, hid)
    out_ref[...] = down_product(hidden, down).astype(out_ref.dtype)


def second_kernel(rows_ref, held, out_ref, *, hid):
    tile = held[:, :, :, : 2 * hid].reshape(-1, 2 * hid)
    both = jnp.dot(rows_ref[...], tile, preferred_element_type=jnp.float32)
    down = held[:, :, :, 2 * hid :].reshape(-1, hid)
    out_ref[...] = down_product(gated_product(both, hid), down).astype(out_ref.dtype)


def ffn_cost(rows, width):
    count, depth = rows.shape
    return pl.CostEstimate(
        flops=2 * count * depth * width,
        bytes_accessed=2 * depth * width + 4 * rows.size,
        transcendentals=count * width // 3,
    )


def feed_forward_first(rows, weights, core):
    count, depth = rows.shape
    width = weights.shape[3]
    vmem = pl.BlockSpec(memory_space=pltpu.VMEM)
    return pl.pallas_call(
        functools.partial(first_kernel, hid=width // 3),
        out_shape=(
            jax.ShapeDtypeStruct((count, depth), jnp.bfloat16),
            jax.ShapeDtypeStruct(weights.shape, weights.dtype),
        ),
        in_specs=[
            pl.BlockSpec(memory_space=pltpu.SMEM),
            vmem,
            pl.BlockSpec(memory_space=pl.ANY),
        ],
        out_specs=(vmem, vmem),
        scratch_shapes=[
            pltpu.VMEM((count, 2 * width // 3), jnp.float32),
            pltpu.SemaphoreType.DMA((2, SIDE)),
        ],
        cost_estimate=ffn_cost(rows, width),
        compiler_params=pltpu.CompilerParams(vmem_limit_bytes=FIRST_VMEM),
        name="ffn_first",
    )(core, rows, weights)


def feed_forward_second(rows, held):
    width = held.shape[3]
    vmem = pl.BlockSpec(memory_space=pltpu.VMEM)
    return pl.pallas_call(
        functools.partial(second_kernel, hid=width // 3),
        out_shape=jax.ShapeDtypeStruct(rows.shape, jnp.float32),
        in_specs=[vmem, vmem],
        out_specs=vmem,
        cost_estimate=ffn_cost(rows, width),
        compiler_params=pltpu.CompilerParams(vmem_limit_bytes=24 * 1024 * 1024),
        name="ffn_second",
    )(rows, held)


def halo_sides(block, axis, width):
    count = lax.axis_size(axis)
    forward = [(i, i + 1) for i in range(count - 1)]
    backward = [(target, source) for source, target in forward]
    low = lax.ppermute(block[:, -width:], axis, forward)
    high = lax.ppermute(block[:, :width], axis, backward)
    return low, high


def attention_kernel(
    place_ref, sink_ref, query_ref, low_ref, mid_ref, high_ref, proj_ref, mate_ref, mine_ref, padded, attended
):
    rows = query_ref.shape[0]
    heads = query_ref.shape[1] // HEAD_DIM
    piece = WINDOW // CORES
    core, start, total = place_ref[0], place_ref[1], place_ref[2]
    padded[:, :WINDOW] = low_ref[...]
    padded[:, WINDOW : WINDOW + rows] = mid_ref[...]
    padded[:, WINDOW + rows :] = high_ref[...]
    query_at = lax.broadcasted_iota(jnp.int32, (WINDOW, 3 * WINDOW), 0)
    key_at = lax.broadcasted_iota(jnp.int32, (WINDOW, 3 * WINDOW), 1)
    near = (key_at >= query_at) & (key_at <= query_at + 2 * WINDOW)
    sink = jnp.concatenate(
        [jnp.full((WINDOW, 1), sink_ref[head], jnp.float32) for head in range(heads)], axis=0
    )
    for block in range(rows // WINDOW):
        at = block * WINDOW
        position = key_at + (start + at - WINDOW)
        valid = near & (position >= 0) & (position < total)
        keys = padded[:HEAD_DIM, at : at + 3 * WINDOW]
        values = padded[HEAD_DIM:, at : at + 3 * WINDOW]
        scaled = query_ref[at : at + WINDOW, :] * jnp.bfloat16(HEAD_DIM ** (-0.5))
        stacked = jnp.concatenate(
            [scaled[:, head * HEAD_DIM : (head + 1) * HEAD_DIM] for head in range(heads)], axis=0
        )
        scores = jnp.dot(stacked, keys, preferred_element_type=jnp.float32)
        scores = jnp.where(jnp.concatenate([valid] * heads, axis=0), scores, -1e30)
        peak = jnp.maximum(jnp.max(scores, axis=1, keepdims=True), sink)
        raw = jnp.exp(scores - peak)
        denom = jnp.sum(raw, axis=1, keepdims=True) + jnp.exp(sink - peak)
        probs = (raw * (1.0 / denom)).astype(jnp.bfloat16)
        mixed = lax.dot_general(
            probs, values, (((1,), (1,)), ((), ())), preferred_element_type=jnp.float32
        ).astype(jnp.bfloat16)
        attended[at : at + WINDOW, :] = jnp.concatenate(
            [mixed[head * WINDOW : (head + 1) * WINDOW] for head in range(heads)], axis=1
        )
    for target, which in ((mate_ref, 1 - core), (mine_ref, core)):
        picked = jnp.concatenate(
            [
                attended[pl.ds(pl.multiple_of(at + which * piece, piece), piece), :]
                for at in range(0, rows, WINDOW)
            ],
            axis=0,
        )
        target[...] = jnp.dot(picked, proj_ref[...], preferred_element_type=jnp.float32).astype(
            target.dtype
        )


def attend_and_project(queries, sides, middle, sink_logit, out_weight, place):
    rows, columns = queries.shape
    depth = out_weight.shape[1]
    low, high = sides
    vmem = pl.BlockSpec(memory_space=pltpu.VMEM)
    smem = pl.BlockSpec(memory_space=pltpu.SMEM)
    half = rows // CORES
    return pl.pallas_call(
        attention_kernel,
        out_shape=(
            jax.ShapeDtypeStruct((half, depth), jnp.bfloat16),
            jax.ShapeDtypeStruct((half, depth), jnp.float32),
        ),
        in_specs=[smem, smem, vmem, vmem, vmem, vmem, vmem],
        out_specs=(vmem, vmem),
        scratch_shapes=[
            pltpu.VMEM((2 * HEAD_DIM, rows + 2 * WINDOW), jnp.bfloat16),
            pltpu.VMEM((rows, columns), jnp.bfloat16),
        ],
        cost_estimate=pl.CostEstimate(
            flops=2 * rows * columns * (6 * WINDOW + depth),
            bytes_accessed=8 * half * depth,
            transcendentals=3 * WINDOW * rows * columns // HEAD_DIM,
        ),
        compiler_params=pltpu.CompilerParams(vmem_limit_bytes=16 * 1024 * 1024),
        name="attend",
    )(place, sink_logit, queries, low, middle, high, out_weight)


def norm_kernel(pieces_ref, residual_ref, gain_ref, mixed_ref, spread_ref):
    mixed = residual_ref[...].astype(jnp.float32)
    mixed += jnp.sum(pieces_ref[...].astype(jnp.float32), axis=0)
    mixed_ref[...] = mixed
    inverse = lax.rsqrt(jnp.mean(mixed * mixed, axis=1, keepdims=True) + 1e-06)
    normed = (mixed * inverse * gain_ref[...]).astype(spread_ref.dtype)
    for i in range(spread_ref.shape[0]):
        spread_ref[i] = normed


def sum_and_norm(pieces, residual, norm_gain):
    vmem = pl.BlockSpec(memory_space=pltpu.VMEM)
    return pl.pallas_call(
        norm_kernel,
        out_shape=(
            jax.ShapeDtypeStruct(residual.shape, jnp.float32),
            jax.ShapeDtypeStruct(pieces.shape, residual.dtype),
        ),
        in_specs=[vmem] * 3,
        out_specs=(vmem, vmem),
        compiler_params=pltpu.CompilerParams(vmem_limit_bytes=8 * 1024 * 1024),
        name="norm",
    )(pieces, residual, norm_gain.reshape(1, -1))


def last_kernel(pieces_ref, mixed_ref, out_ref):
    total = mixed_ref[...] + jnp.sum(pieces_ref[...].astype(jnp.float32), axis=0)
    out_ref[...] = total.astype(out_ref.dtype)


def last_sum(pieces, mixed):
    vmem = pl.BlockSpec(memory_space=pltpu.VMEM)
    return pl.pallas_call(
        last_kernel,
        out_shape=jax.ShapeDtypeStruct(mixed.shape, pieces.dtype),
        in_specs=[vmem] * 2,
        out_specs=vmem,
        compiler_params=pltpu.CompilerParams(vmem_limit_bytes=8 * 1024 * 1024),
        name="last",
    )(pieces, mixed)


def shards(
    queries,
    key_rows,
    values,
    sink_logit,
    residual_in,
    out_weight,
    norm_gain,
    gate_weight,
    up_weight,
    down_weight,
):
    rows_here, depth = queries.shape[0], residual_in.shape[1]
    sps, tps = lax.axis_size("sp"), lax.axis_size("tp")
    xs = tps // CORES
    own = rows_here // tps
    core = lax.axis_index("tp") % CORES
    both_axes = ("sp", "tp")

    mine = jnp.concatenate([gate_weight, up_weight, down_weight.T], axis=1)
    line = lax.all_to_all(
        jnp.broadcast_to(mine[None], (SIDE, *mine.shape)),
        both_axes,
        0,
        0,
        tiled=True,
        axis_index_groups=line_groups(sps, tps, True),
    )
    line, queries, key_rows, values = lax.optimization_barrier((line, queries, key_rows, values))
    weights = lax.all_gather(
        line, both_axes, axis=0, tiled=False, axis_index_groups=line_groups(sps, tps, False)
    )

    middle = jnp.concatenate([key_rows.T, values.T], axis=0)
    sides = halo_sides(middle, "sp", WINDOW)
    place = jnp.stack([core, lax.axis_index("sp") * rows_here, jnp.int32(rows_here * sps)]).astype(
        jnp.int32
    )

    def swap(array):
        return lax.ppermute(array, "tp", core_swap(tps))

    def exchange(blocks):
        return lax.all_to_all(
            blocks.reshape(xs, own, depth), "tp", 0, 0, tiled=True, axis_index_groups=x_groups(tps)
        )

    def added(mine, mates):
        return exchange((mine + mates.astype(jnp.float32)).astype(jnp.bfloat16))

    mate_part, my_part = attend_and_project(
        queries, sides, middle, sink_logit, out_weight, place
    )
    mixed_rows, spread = sum_and_norm(added(my_part, swap(mate_part)), residual_in, norm_gain)
    my_rows = exchange(spread).reshape(xs * own, depth)
    mate_rows = swap(my_rows)
    mate_out, held = feed_forward_first(mate_rows, weights, core.astype(jnp.int32).reshape(1))
    mate_sum = swap(mate_out)
    my_out = feed_forward_second(my_rows, held)
    return last_sum(added(my_out, mate_sum), mixed_rows)


def solution(mesh):
    return jax.shard_map(
        shards,
        mesh=mesh,
        in_specs=(
            P("sp", "tp"),
            P("sp", "tp"),
            P("sp", "tp"),
            P("tp"),
            P(("sp", "tp"), None),
            P("tp", None),
            P(),
            P("sp", "tp"),
            P("sp", "tp"),
            P("tp", "sp"),
        ),
        out_specs=P(("sp", "tp"), None),
        check_vma=False,
    )
```

```python
import functools

import jax
import jax.numpy as jnp
from jax import lax
from jax.experimental import pallas as pl
from jax.experimental.pallas import tpu as pltpu
from jax.sharding import PartitionSpec as P

HEAD_DIM = 64
WINDOW = 128
SIDE = 8
CORES = 2
LANES = 128
FIRST_VMEM = 40 * 1024 * 1024


def device_index(sp, tp, tps):
    return sp * tps + tp


def line_groups(sps, tps, first):
    groups = []
    for tp in range(tps):
        along_y = (tp % CORES == 0) == first
        for fixed in range(sps // SIDE):
            line = [fixed * SIDE + k if along_y else k * SIDE + fixed for k in range(SIDE)]
            groups.append([device_index(sp, tp, tps) for sp in line])
    return groups


def x_groups(tps):
    return [[x * CORES + core for x in range(tps // CORES)] for core in range(CORES)]


def core_swap(tps):
    return [(i, i ^ 1) for i in range(tps)]


def pack_kernel(joined_ref, out_ref):
    piece, width = joined_ref.shape
    whole = width // LANES
    rows = [joined_ref[:, i * LANES : (i + 1) * LANES] for i in range(whole)]
    last = joined_ref[:, whole * LANES :]
    rows.append(jnp.concatenate([last[: piece // 2], last[piece // 2 :]], axis=1))
    packed = jnp.concatenate(rows, axis=0)
    for i in range(out_ref.shape[0]):
        out_ref[i] = packed


def pack_copies(joined):
    piece, width = joined.shape
    vmem = pl.BlockSpec(memory_space=pltpu.VMEM)
    return pl.pallas_call(
        pack_kernel,
        out_shape=jax.ShapeDtypeStruct((SIDE, piece * width // LANES, LANES), joined.dtype),
        in_specs=[vmem],
        out_specs=vmem,
        compiler_params=pltpu.CompilerParams(vmem_limit_bytes=4 * 1024 * 1024),
        name="pack",
    )(joined)


def gate_up(held, first, count, piece, hid):
    tiles = [
        held[first : first + count, :, i * piece : (i + 1) * piece, :].reshape(-1, LANES)
        for i in range(2 * hid // LANES)
    ]
    return jnp.concatenate(tiles, axis=1)


def down_matrix(held, piece, hid):
    tiles = [
        held[:, :, i * piece : (i + 1) * piece, :].reshape(-1, LANES)
        for i in range(2 * hid // LANES, 3 * hid // LANES)
    ]
    last = held[:, :, 3 * hid // LANES * piece :, :].reshape(SIDE * SIDE, piece // 2, LANES)
    last = jnp.concatenate([last[:, :, : LANES // 2], last[:, :, LANES // 2 :]], axis=1)
    return jnp.concatenate(tiles + [last.reshape(-1, LANES // 2)], axis=1)


def gated_product(both, hid):
    gate, up = both[:, :hid], both[:, hid:]
    return (gate / (1.0 + jnp.exp(-gate)) * up).astype(jnp.bfloat16)


def down_product(hidden, down):
    return lax.dot_general(hidden, down, (((1,), (1,)), ((), ())), preferred_element_type=jnp.float32)


def first_kernel(core_ref, rows_ref, weights_ref, out_ref, held, total, sems, *, piece, hid):
    per = 2
    span = per * SIDE * piece
    down_at = 2 * hid // LANES * piece
    core = core_ref[0]

    def copy(i, swapped, part):
        lines = (pl.ds(0, down_at), pl.ds(down_at, held.shape[2] - down_at))[part]
        source = weights_ref.at[:, i, lines] if swapped else weights_ref.at[i, :, lines]
        return pltpu.make_async_copy(source, held.at[i, :, lines], sems.at[part, i])

    for swapped in (False, True):

        @pl.when(core == int(swapped))
        def _():
            for part in range(2):
                for i in range(SIDE):
                    copy(i, swapped, part).start()

    both = None
    for step in range(SIDE // per):
        for i in range(step * per, (step + 1) * per):
            copy(i, False, 0).wait()
        part = jnp.dot(
            rows_ref[:, step * span : (step + 1) * span],
            gate_up(held, step * per, per, piece, hid),
            preferred_element_type=jnp.float32,
        )
        if step == 0:
            total[...] = part
        elif step < SIDE // per - 1:
            total[...] += part
        else:
            both = total[...] + part
    hidden = gated_product(both, hid)
    for i in range(SIDE):
        copy(i, False, 1).wait()
    out_ref[...] = down_product(hidden, down_matrix(held, piece, hid)).astype(out_ref.dtype)


def second_kernel(rows_ref, held, out_ref, *, piece, hid):
    both = jnp.dot(
        rows_ref[...], gate_up(held, 0, SIDE, piece, hid), preferred_element_type=jnp.float32
    )
    out_ref[...] = down_product(gated_product(both, hid), down_matrix(held, piece, hid)).astype(
        out_ref.dtype
    )


def ffn_cost(rows, width):
    count, depth = rows.shape
    return pl.CostEstimate(
        flops=2 * count * depth * width,
        bytes_accessed=2 * depth * width + 4 * rows.size,
        transcendentals=count * width // 3,
    )


def feed_forward_first(rows, weights, core, piece, width):
    count, depth = rows.shape
    vmem = pl.BlockSpec(memory_space=pltpu.VMEM)
    return pl.pallas_call(
        functools.partial(first_kernel, piece=piece, hid=width // 3),
        out_shape=(
            jax.ShapeDtypeStruct((count, depth), jnp.bfloat16),
            jax.ShapeDtypeStruct(weights.shape, weights.dtype),
        ),
        in_specs=[
            pl.BlockSpec(memory_space=pltpu.SMEM),
            vmem,
            pl.BlockSpec(memory_space=pl.ANY),
        ],
        out_specs=(vmem, vmem),
        scratch_shapes=[
            pltpu.VMEM((count, 2 * width // 3), jnp.float32),
            pltpu.SemaphoreType.DMA((2, SIDE)),
        ],
        cost_estimate=ffn_cost(rows, width),
        compiler_params=pltpu.CompilerParams(vmem_limit_bytes=FIRST_VMEM),
        name="ffn_first",
    )(core, rows, weights)


def feed_forward_second(rows, held, piece, width):
    vmem = pl.BlockSpec(memory_space=pltpu.VMEM)
    return pl.pallas_call(
        functools.partial(second_kernel, piece=piece, hid=width // 3),
        out_shape=jax.ShapeDtypeStruct(rows.shape, jnp.float32),
        in_specs=[vmem, vmem],
        out_specs=vmem,
        cost_estimate=ffn_cost(rows, width),
        compiler_params=pltpu.CompilerParams(vmem_limit_bytes=24 * 1024 * 1024),
        name="ffn_second",
    )(rows, held)


def halo_sides(block, axis, width):
    count = lax.axis_size(axis)
    forward = [(i, i + 1) for i in range(count - 1)]
    backward = [(target, source) for source, target in forward]
    low = lax.ppermute(block[:, -width:], axis, forward)
    high = lax.ppermute(block[:, :width], axis, backward)
    return low, high


def attention_kernel(
    place_ref, sink_ref, query_ref, low_ref, mid_ref, high_ref, proj_ref, mate_ref, mine_ref, padded, attended
):
    rows = query_ref.shape[0]
    heads = query_ref.shape[1] // HEAD_DIM
    piece = WINDOW // CORES
    core, start, total = place_ref[0], place_ref[1], place_ref[2]
    padded[:, :WINDOW] = low_ref[...]
    padded[:, WINDOW : WINDOW + rows] = mid_ref[...]
    padded[:, WINDOW + rows :] = high_ref[...]
    query_at = lax.broadcasted_iota(jnp.int32, (WINDOW, 3 * WINDOW), 0)
    key_at = lax.broadcasted_iota(jnp.int32, (WINDOW, 3 * WINDOW), 1)
    near = (key_at >= query_at) & (key_at <= query_at + 2 * WINDOW)
    sink = jnp.concatenate(
        [jnp.full((WINDOW, 1), sink_ref[head], jnp.float32) for head in range(heads)], axis=0
    )
    for block in range(rows // WINDOW):
        at = block * WINDOW
        position = key_at + (start + at - WINDOW)
        valid = near & (position >= 0) & (position < total)
        keys = padded[:HEAD_DIM, at : at + 3 * WINDOW]
        values = padded[HEAD_DIM:, at : at + 3 * WINDOW]
        scaled = query_ref[at : at + WINDOW, :] * jnp.bfloat16(HEAD_DIM ** (-0.5))
        stacked = jnp.concatenate(
            [scaled[:, head * HEAD_DIM : (head + 1) * HEAD_DIM] for head in range(heads)], axis=0
        )
        scores = jnp.dot(stacked, keys, preferred_element_type=jnp.float32)
        scores = jnp.where(jnp.concatenate([valid] * heads, axis=0), scores, -1e30)
        peak = jnp.maximum(jnp.max(scores, axis=1, keepdims=True), sink)
        raw = jnp.exp(scores - peak)
        denom = jnp.sum(raw, axis=1, keepdims=True) + jnp.exp(sink - peak)
        probs = (raw * (1.0 / denom)).astype(jnp.bfloat16)
        mixed = lax.dot_general(
            probs, values, (((1,), (1,)), ((), ())), preferred_element_type=jnp.float32
        ).astype(jnp.bfloat16)
        attended[at : at + WINDOW, :] = jnp.concatenate(
            [mixed[head * WINDOW : (head + 1) * WINDOW] for head in range(heads)], axis=1
        )
    for target, which in ((mate_ref, 1 - core), (mine_ref, core)):
        picked = jnp.concatenate(
            [
                attended[pl.ds(pl.multiple_of(at + which * piece, piece), piece), :]
                for at in range(0, rows, WINDOW)
            ],
            axis=0,
        )
        target[...] = jnp.dot(picked, proj_ref[...], preferred_element_type=jnp.float32).astype(
            target.dtype
        )


def attend_and_project(queries, sides, middle, sink_logit, out_weight, place):
    rows, columns = queries.shape
    depth = out_weight.shape[1]
    low, high = sides
    vmem = pl.BlockSpec(memory_space=pltpu.VMEM)
    smem = pl.BlockSpec(memory_space=pltpu.SMEM)
    half = rows // CORES
    return pl.pallas_call(
        attention_kernel,
        out_shape=(
            jax.ShapeDtypeStruct((half, depth), jnp.bfloat16),
            jax.ShapeDtypeStruct((half, depth), jnp.float32),
        ),
        in_specs=[smem, smem, vmem, vmem, vmem, vmem, vmem],
        out_specs=(vmem, vmem),
        scratch_shapes=[
            pltpu.VMEM((2 * HEAD_DIM, rows + 2 * WINDOW), jnp.bfloat16),
            pltpu.VMEM((rows, columns), jnp.bfloat16),
        ],
        cost_estimate=pl.CostEstimate(
            flops=2 * rows * columns * (6 * WINDOW + depth),
            bytes_accessed=8 * half * depth,
            transcendentals=3 * WINDOW * rows * columns // HEAD_DIM,
        ),
        compiler_params=pltpu.CompilerParams(vmem_limit_bytes=16 * 1024 * 1024),
        name="attend",
    )(place, sink_logit, queries, low, middle, high, out_weight)


def norm_kernel(pieces_ref, residual_ref, gain_ref, mixed_ref, spread_ref):
    mixed = residual_ref[...].astype(jnp.float32)
    mixed += jnp.sum(pieces_ref[...].astype(jnp.float32), axis=0)
    mixed_ref[...] = mixed
    inverse = lax.rsqrt(jnp.mean(mixed * mixed, axis=1, keepdims=True) + 1e-06)
    normed = (mixed * inverse * gain_ref[...]).astype(spread_ref.dtype)
    for i in range(spread_ref.shape[0]):
        spread_ref[i] = normed


def sum_and_norm(pieces, residual, norm_gain):
    vmem = pl.BlockSpec(memory_space=pltpu.VMEM)
    return pl.pallas_call(
        norm_kernel,
        out_shape=(
            jax.ShapeDtypeStruct(residual.shape, jnp.float32),
            jax.ShapeDtypeStruct(pieces.shape, residual.dtype),
        ),
        in_specs=[vmem] * 3,
        out_specs=(vmem, vmem),
        compiler_params=pltpu.CompilerParams(vmem_limit_bytes=8 * 1024 * 1024),
        name="norm",
    )(pieces, residual, norm_gain.reshape(1, -1))


def last_kernel(pieces_ref, mixed_ref, out_ref):
    total = mixed_ref[...] + jnp.sum(pieces_ref[...].astype(jnp.float32), axis=0)
    out_ref[...] = total.astype(out_ref.dtype)


def last_sum(pieces, mixed):
    vmem = pl.BlockSpec(memory_space=pltpu.VMEM)
    return pl.pallas_call(
        last_kernel,
        out_shape=jax.ShapeDtypeStruct(mixed.shape, pieces.dtype),
        in_specs=[vmem] * 2,
        out_specs=vmem,
        compiler_params=pltpu.CompilerParams(vmem_limit_bytes=8 * 1024 * 1024),
        name="last",
    )(pieces, mixed)


def shards(
    queries,
    key_rows,
    values,
    sink_logit,
    residual_in,
    out_weight,
    norm_gain,
    gate_weight,
    up_weight,
    down_weight,
):
    rows_here, depth = queries.shape[0], residual_in.shape[1]
    sps, tps = lax.axis_size("sp"), lax.axis_size("tp")
    xs = tps // CORES
    own = rows_here // tps
    core = lax.axis_index("tp") % CORES
    both_axes = ("sp", "tp")

    mine = jnp.concatenate([gate_weight, up_weight, down_weight.T], axis=1)
    line = lax.all_to_all(
        pack_copies(mine),
        both_axes,
        0,
        0,
        tiled=True,
        axis_index_groups=line_groups(sps, tps, True),
    )
    line, queries, key_rows, values = lax.optimization_barrier((line, queries, key_rows, values))
    weights = lax.all_gather(
        line, both_axes, axis=0, tiled=False, axis_index_groups=line_groups(sps, tps, False)
    )

    middle = jnp.concatenate([key_rows.T, values.T], axis=0)
    sides = halo_sides(middle, "sp", WINDOW)
    place = jnp.stack([core, lax.axis_index("sp") * rows_here, jnp.int32(rows_here * sps)]).astype(
        jnp.int32
    )

    def swap(array):
        return lax.ppermute(array, "tp", core_swap(tps))

    def exchange(blocks):
        return lax.all_to_all(
            blocks.reshape(xs, own, depth), "tp", 0, 0, tiled=True, axis_index_groups=x_groups(tps)
        )

    def added(mine, mates):
        return exchange((mine + mates.astype(jnp.float32)).astype(jnp.bfloat16))

    mate_part, my_part = attend_and_project(
        queries, sides, middle, sink_logit, out_weight, place
    )
    mixed_rows, spread = sum_and_norm(added(my_part, swap(mate_part)), residual_in, norm_gain)
    my_rows = exchange(spread).reshape(xs * own, depth)
    mate_rows = swap(my_rows)
    mate_out, held = feed_forward_first(
        mate_rows, weights, core.astype(jnp.int32).reshape(1), *mine.shape
    )
    mate_sum = swap(mate_out)
    my_out = feed_forward_second(my_rows, held, *mine.shape)
    return last_sum(added(my_out, mate_sum), mixed_rows)


def solution(mesh):
    return jax.shard_map(
        shards,
        mesh=mesh,
        in_specs=(
            P("sp", "tp"),
            P("sp", "tp"),
            P("sp", "tp"),
            P("tp"),
            P(("sp", "tp"), None),
            P("tp", None),
            P(),
            P("sp", "tp"),
            P("sp", "tp"),
            P("tp", "sp"),
        ),
        out_specs=P(("sp", "tp"), None),
        check_vma=False,
    )
```

```python
import functools

import jax
import jax.numpy as jnp
from jax import lax
from jax.experimental import pallas as pl
from jax.experimental.pallas import tpu as pltpu
from jax.sharding import PartitionSpec as P

HEAD_DIM = 64
WINDOW = 128
SIDE = 8
CORES = 2
LANES = 128
FIRST_VMEM = 40 * 1024 * 1024


def device_index(sp, tp, tps):
    return sp * tps + tp


def line_groups(sps, tps, first):
    groups = []
    for tp in range(tps):
        along_y = (tp % CORES == 0) == first
        for fixed in range(sps // SIDE):
            line = [fixed * SIDE + k if along_y else k * SIDE + fixed for k in range(SIDE)]
            groups.append([device_index(sp, tp, tps) for sp in line])
    return groups


def x_groups(tps):
    return [[x * CORES + core for x in range(tps // CORES)] for core in range(CORES)]


def core_swap(tps):
    return [(i, i ^ 1) for i in range(tps)]


def pack_kernel(joined_ref, out_ref):
    piece, width = joined_ref.shape
    whole = width // LANES
    rows = [joined_ref[:, i * LANES : (i + 1) * LANES] for i in range(whole)]
    last = joined_ref[:, whole * LANES :]
    rows.append(jnp.concatenate([last[: piece // 2], last[piece // 2 :]], axis=1))
    packed = jnp.concatenate(rows, axis=0)
    for i in range(out_ref.shape[0]):
        out_ref[i] = packed


def pack_copies(joined):
    piece, width = joined.shape
    vmem = pl.BlockSpec(memory_space=pltpu.VMEM)
    return pl.pallas_call(
        pack_kernel,
        out_shape=jax.ShapeDtypeStruct((SIDE, piece * width // LANES, LANES), joined.dtype),
        in_specs=[vmem],
        out_specs=vmem,
        compiler_params=pltpu.CompilerParams(vmem_limit_bytes=4 * 1024 * 1024),
        name="pack",
    )(joined)


def gate_up(held, first, count, piece, hid):
    tiles = [
        held[first : first + count, :, i * piece : (i + 1) * piece, :].reshape(-1, LANES)
        for i in range(2 * hid // LANES)
    ]
    return jnp.concatenate(tiles, axis=1)


def down_matrix(held, piece, hid):
    tiles = [
        held[:, :, i * piece : (i + 1) * piece, :].reshape(-1, LANES)
        for i in range(2 * hid // LANES, 3 * hid // LANES)
    ]
    last = held[:, :, 3 * hid // LANES * piece :, :].reshape(SIDE * SIDE, piece // 2, LANES)
    last = jnp.concatenate([last[:, :, : LANES // 2], last[:, :, LANES // 2 :]], axis=1)
    return jnp.concatenate(tiles + [last.reshape(-1, LANES // 2)], axis=1)


def gated_product(both, hid):
    gate, up = both[:, :hid], both[:, hid:]
    return (gate / (1.0 + jnp.exp(-gate)) * up).astype(jnp.bfloat16)


def down_product(hidden, down):
    return lax.dot_general(hidden, down, (((1,), (1,)), ((), ())), preferred_element_type=jnp.float32)


def first_kernel(core_ref, rows_ref, weights_ref, out_ref, held, total, sems, *, piece, hid):
    per = 2
    span = per * SIDE * piece
    down_at = 2 * hid // LANES * piece
    core = core_ref[0]

    def copy(i, swapped, part):
        lines = (pl.ds(0, down_at), pl.ds(down_at, held.shape[2] - down_at))[part]
        source = weights_ref.at[:, i, lines] if swapped else weights_ref.at[i, :, lines]
        return pltpu.make_async_copy(source, held.at[i, :, lines], sems.at[part, i])

    for swapped in (False, True):

        @pl.when(core == int(swapped))
        def _():
            for part in range(2):
                for i in range(SIDE):
                    copy(i, swapped, part).start()

    both = None
    for step in range(SIDE // per):
        for i in range(step * per, (step + 1) * per):
            copy(i, False, 0).wait()
        part = jnp.dot(
            rows_ref[:, step * span : (step + 1) * span],
            gate_up(held, step * per, per, piece, hid),
            preferred_element_type=jnp.float32,
        )
        if step == 0:
            total[...] = part
        elif step < SIDE // per - 1:
            total[...] += part
        else:
            both = total[...] + part
    hidden = gated_product(both, hid)
    for i in range(SIDE):
        copy(i, False, 1).wait()
    out_ref[...] = down_product(hidden, down_matrix(held, piece, hid)).astype(out_ref.dtype)


def second_kernel(rows_ref, held, out_ref, *, piece, hid):
    both = jnp.dot(
        rows_ref[...], gate_up(held, 0, SIDE, piece, hid), preferred_element_type=jnp.float32
    )
    out_ref[...] = down_product(gated_product(both, hid), down_matrix(held, piece, hid)).astype(
        out_ref.dtype
    )


def ffn_cost(rows, width):
    count, depth = rows.shape
    return pl.CostEstimate(
        flops=2 * count * depth * width,
        bytes_accessed=2 * depth * width + 4 * rows.size,
        transcendentals=count * width // 3,
    )


def feed_forward_first(rows, weights, core, piece, width):
    count, depth = rows.shape
    vmem = pl.BlockSpec(memory_space=pltpu.VMEM)
    return pl.pallas_call(
        functools.partial(first_kernel, piece=piece, hid=width // 3),
        out_shape=(
            jax.ShapeDtypeStruct((count, depth), jnp.bfloat16),
            jax.ShapeDtypeStruct(weights.shape, weights.dtype),
        ),
        in_specs=[
            pl.BlockSpec(memory_space=pltpu.SMEM),
            vmem,
            pl.BlockSpec(memory_space=pl.ANY),
        ],
        out_specs=(vmem, vmem),
        scratch_shapes=[
            pltpu.VMEM((count, 2 * width // 3), jnp.float32),
            pltpu.SemaphoreType.DMA((2, SIDE)),
        ],
        cost_estimate=ffn_cost(rows, width),
        compiler_params=pltpu.CompilerParams(vmem_limit_bytes=FIRST_VMEM),
        name="ffn_first",
    )(core, rows, weights)


def feed_forward_second(rows, held, piece, width):
    vmem = pl.BlockSpec(memory_space=pltpu.VMEM)
    return pl.pallas_call(
        functools.partial(second_kernel, piece=piece, hid=width // 3),
        out_shape=jax.ShapeDtypeStruct(rows.shape, jnp.float32),
        in_specs=[vmem, vmem],
        out_specs=vmem,
        cost_estimate=ffn_cost(rows, width),
        compiler_params=pltpu.CompilerParams(vmem_limit_bytes=24 * 1024 * 1024),
        name="ffn_second",
    )(rows, held)


def halo_sides(block, axis, width):
    count = lax.axis_size(axis)
    forward = [(i, i + 1) for i in range(count - 1)]
    backward = [(target, source) for source, target in forward]
    low = lax.ppermute(block[:, -width:], axis, forward)
    high = lax.ppermute(block[:, :width], axis, backward)
    return low, high


def attend_block(query, band, valid, sink):
    heads = query.shape[1] // HEAD_DIM
    scaled = query * jnp.bfloat16(HEAD_DIM ** (-0.5))
    stacked = jnp.concatenate(
        [scaled[:, head * HEAD_DIM : (head + 1) * HEAD_DIM] for head in range(heads)], axis=0
    )
    scores = jnp.dot(stacked, band[:HEAD_DIM], preferred_element_type=jnp.float32)
    scores = jnp.where(jnp.concatenate([valid] * heads, axis=0), scores, -1e30)
    peak = jnp.maximum(jnp.max(scores, axis=1, keepdims=True), sink)
    raw = jnp.exp(scores - peak)
    denom = jnp.sum(raw, axis=1, keepdims=True) + jnp.exp(sink - peak)
    probs = (raw * (1.0 / denom)).astype(jnp.bfloat16)
    mixed = lax.dot_general(
        probs, band[HEAD_DIM:], (((1,), (1,)), ((), ())), preferred_element_type=jnp.float32
    ).astype(jnp.bfloat16)
    return jnp.concatenate(
        [mixed[head * WINDOW : (head + 1) * WINDOW] for head in range(heads)], axis=1
    )


def near_and_position():
    query_at = lax.broadcasted_iota(jnp.int32, (WINDOW, 3 * WINDOW), 0)
    key_at = lax.broadcasted_iota(jnp.int32, (WINDOW, 3 * WINDOW), 1)
    return (key_at >= query_at) & (key_at <= query_at + 2 * WINDOW), key_at


def sink_column(sink_ref, heads):
    return jnp.concatenate(
        [jnp.full((WINDOW, 1), sink_ref[head], jnp.float32) for head in range(heads)], axis=0
    )


def inner_kernel(sink_ref, query_ref, mid_ref, out_ref):
    near, _ = near_and_position()
    sink = sink_column(sink_ref, query_ref.shape[1] // HEAD_DIM)
    for at in range(WINDOW, query_ref.shape[0] - WINDOW, WINDOW):
        out_ref[at - WINDOW : at, :] = attend_block(
            query_ref[at : at + WINDOW, :], mid_ref[:, at - WINDOW : at + 2 * WINDOW], near, sink
        )


def attend_inner(queries, middle, sink_logit):
    rows, columns = queries.shape
    vmem = pl.BlockSpec(memory_space=pltpu.VMEM)
    return pl.pallas_call(
        inner_kernel,
        out_shape=jax.ShapeDtypeStruct((rows - 2 * WINDOW, columns), queries.dtype),
        in_specs=[pl.BlockSpec(memory_space=pltpu.SMEM), vmem, vmem],
        out_specs=vmem,
        cost_estimate=pl.CostEstimate(
            flops=12 * WINDOW * rows * columns,
            bytes_accessed=4 * rows * columns,
            transcendentals=WINDOW * rows * columns // HEAD_DIM,
        ),
        compiler_params=pltpu.CompilerParams(vmem_limit_bytes=16 * 1024 * 1024),
        name="inner",
    )(sink_logit, queries, middle)


def attention_kernel(
    place_ref, sink_ref, query_ref, low_ref, mid_ref, high_ref, inner_ref, proj_ref, mate_ref, mine_ref, attended
):
    rows = query_ref.shape[0]
    piece = WINDOW // CORES
    core, start, total = place_ref[0], place_ref[1], place_ref[2]
    near, key_at = near_and_position()
    sink = sink_column(sink_ref, query_ref.shape[1] // HEAD_DIM)
    first = jnp.concatenate([low_ref[...], mid_ref[:, : 2 * WINDOW]], axis=1)
    last = jnp.concatenate([mid_ref[:, rows - 2 * WINDOW :], high_ref[...]], axis=1)
    for at, band in ((0, first), (rows - WINDOW, last)):
        position = key_at + (start + at - WINDOW)
        valid = near & (position >= 0) & (position < total)
        attended[at : at + WINDOW, :] = attend_block(
            query_ref[at : at + WINDOW, :], band, valid, sink
        )
    attended[WINDOW : rows - WINDOW, :] = inner_ref[...]
    for target, which in ((mate_ref, 1 - core), (mine_ref, core)):
        picked = jnp.concatenate(
            [
                attended[pl.ds(pl.multiple_of(at + which * piece, piece), piece), :]
                for at in range(0, rows, WINDOW)
            ],
            axis=0,
        )
        target[...] = jnp.dot(picked, proj_ref[...], preferred_element_type=jnp.float32).astype(
            target.dtype
        )


def attend_and_project(queries, sides, middle, inner, sink_logit, out_weight, place):
    rows, columns = queries.shape
    depth = out_weight.shape[1]
    low, high = sides
    vmem = pl.BlockSpec(memory_space=pltpu.VMEM)
    smem = pl.BlockSpec(memory_space=pltpu.SMEM)
    half = rows // CORES
    return pl.pallas_call(
        attention_kernel,
        out_shape=(
            jax.ShapeDtypeStruct((half, depth), jnp.bfloat16),
            jax.ShapeDtypeStruct((half, depth), jnp.float32),
        ),
        in_specs=[smem, smem] + [vmem] * 6,
        out_specs=(vmem, vmem),
        scratch_shapes=[pltpu.VMEM((rows, columns), jnp.bfloat16)],
        cost_estimate=pl.CostEstimate(
            flops=2 * rows * columns * (6 * WINDOW + depth),
            bytes_accessed=8 * half * depth,
            transcendentals=3 * WINDOW * rows * columns // HEAD_DIM,
        ),
        compiler_params=pltpu.CompilerParams(vmem_limit_bytes=16 * 1024 * 1024),
        name="attend",
    )(place, sink_logit, queries, low, middle, high, inner, out_weight)


def norm_kernel(pieces_ref, residual_ref, gain_ref, mixed_ref, spread_ref):
    mixed = residual_ref[...].astype(jnp.float32)
    mixed += jnp.sum(pieces_ref[...].astype(jnp.float32), axis=0)
    mixed_ref[...] = mixed
    inverse = lax.rsqrt(jnp.mean(mixed * mixed, axis=1, keepdims=True) + 1e-06)
    normed = (mixed * inverse * gain_ref[...]).astype(spread_ref.dtype)
    for i in range(spread_ref.shape[0]):
        spread_ref[i] = normed


def sum_and_norm(pieces, residual, norm_gain):
    vmem = pl.BlockSpec(memory_space=pltpu.VMEM)
    return pl.pallas_call(
        norm_kernel,
        out_shape=(
            jax.ShapeDtypeStruct(residual.shape, jnp.float32),
            jax.ShapeDtypeStruct(pieces.shape, residual.dtype),
        ),
        in_specs=[vmem] * 3,
        out_specs=(vmem, vmem),
        compiler_params=pltpu.CompilerParams(vmem_limit_bytes=8 * 1024 * 1024),
        name="norm",
    )(pieces, residual, norm_gain.reshape(1, -1))


def last_kernel(pieces_ref, mixed_ref, out_ref):
    total = mixed_ref[...] + jnp.sum(pieces_ref[...].astype(jnp.float32), axis=0)
    out_ref[...] = total.astype(out_ref.dtype)


def last_sum(pieces, mixed):
    vmem = pl.BlockSpec(memory_space=pltpu.VMEM)
    return pl.pallas_call(
        last_kernel,
        out_shape=jax.ShapeDtypeStruct(mixed.shape, pieces.dtype),
        in_specs=[vmem] * 2,
        out_specs=vmem,
        compiler_params=pltpu.CompilerParams(vmem_limit_bytes=8 * 1024 * 1024),
        name="last",
    )(pieces, mixed)


def shards(
    queries,
    key_rows,
    values,
    sink_logit,
    residual_in,
    out_weight,
    norm_gain,
    gate_weight,
    up_weight,
    down_weight,
):
    rows_here, depth = queries.shape[0], residual_in.shape[1]
    sps, tps = lax.axis_size("sp"), lax.axis_size("tp")
    xs = tps // CORES
    own = rows_here // tps
    core = lax.axis_index("tp") % CORES
    both_axes = ("sp", "tp")

    mine = jnp.concatenate([gate_weight, up_weight, down_weight.T], axis=1)
    line = lax.all_to_all(
        pack_copies(mine),
        both_axes,
        0,
        0,
        tiled=True,
        axis_index_groups=line_groups(sps, tps, True),
    )
    line, queries, key_rows, values = lax.optimization_barrier((line, queries, key_rows, values))
    weights = lax.all_gather(
        line, both_axes, axis=0, tiled=False, axis_index_groups=line_groups(sps, tps, False)
    )

    middle = jnp.concatenate([key_rows.T, values.T], axis=0)
    sides = halo_sides(middle, "sp", WINDOW)
    place = jnp.stack([core, lax.axis_index("sp") * rows_here, jnp.int32(rows_here * sps)]).astype(
        jnp.int32
    )

    def swap(array):
        return lax.ppermute(array, "tp", core_swap(tps))

    def exchange(blocks):
        return lax.all_to_all(
            blocks.reshape(xs, own, depth), "tp", 0, 0, tiled=True, axis_index_groups=x_groups(tps)
        )

    def added(mine, mates):
        return exchange((mine + mates.astype(jnp.float32)).astype(jnp.bfloat16))

    mate_part, my_part = attend_and_project(
        queries, sides, middle, attend_inner(queries, middle, sink_logit), sink_logit, out_weight, place
    )
    mixed_rows, spread = sum_and_norm(added(my_part, swap(mate_part)), residual_in, norm_gain)
    my_rows = exchange(spread).reshape(xs * own, depth)
    mate_rows = swap(my_rows)
    mate_out, held = feed_forward_first(
        mate_rows, weights, core.astype(jnp.int32).reshape(1), *mine.shape
    )
    mate_sum = swap(mate_out)
    my_out = feed_forward_second(my_rows, held, *mine.shape)
    return last_sum(added(my_out, mate_sum), mixed_rows)


def solution(mesh):
    return jax.shard_map(
        shards,
        mesh=mesh,
        in_specs=(
            P("sp", "tp"),
            P("sp", "tp"),
            P("sp", "tp"),
            P("tp"),
            P(("sp", "tp"), None),
            P("tp", None),
            P(),
            P("sp", "tp"),
            P("sp", "tp"),
            P("tp", "sp"),
        ),
        out_specs=P(("sp", "tp"), None),
        check_vma=False,
    )
```

```python
import functools

import jax
import jax.numpy as jnp
from jax import lax
from jax.experimental import pallas as pl
from jax.experimental.pallas import tpu as pltpu
from jax.sharding import PartitionSpec as P

HEAD_DIM = 64
WINDOW = 128
SIDE = 8
CORES = 2
LANES = 128
FIRST_VMEM = 40 * 1024 * 1024


def device_index(sp, tp, tps):
    return sp * tps + tp


def line_groups(sps, tps, first):
    groups = []
    for tp in range(tps):
        along_y = (tp % CORES == 0) == first
        for fixed in range(sps // SIDE):
            line = [fixed * SIDE + k if along_y else k * SIDE + fixed for k in range(SIDE)]
            groups.append([device_index(sp, tp, tps) for sp in line])
    return groups


def x_groups(tps):
    return [[x * CORES + core for x in range(tps // CORES)] for core in range(CORES)]


def core_swap(tps):
    return [(i, i ^ 1) for i in range(tps)]


def pack_kernel(joined_ref, out_ref):
    piece, width = joined_ref.shape
    whole = width // LANES
    rows = [joined_ref[:, i * LANES : (i + 1) * LANES] for i in range(whole)]
    last = joined_ref[:, whole * LANES :]
    rows.append(jnp.concatenate([last[: piece // 2], last[piece // 2 :]], axis=1))
    packed = jnp.concatenate(rows, axis=0)
    for i in range(out_ref.shape[0]):
        out_ref[i] = packed


def pack_copies(joined):
    piece, width = joined.shape
    vmem = pl.BlockSpec(memory_space=pltpu.VMEM)
    return pl.pallas_call(
        pack_kernel,
        out_shape=jax.ShapeDtypeStruct((SIDE, piece * width // LANES, LANES), joined.dtype),
        in_specs=[vmem],
        out_specs=vmem,
        compiler_params=pltpu.CompilerParams(vmem_limit_bytes=4 * 1024 * 1024),
        name="pack",
    )(joined)


def gate_up(held, first, count, piece, hid):
    tiles = [
        held[first : first + count, :, i * piece : (i + 1) * piece, :].reshape(-1, LANES)
        for i in range(2 * hid // LANES)
    ]
    return jnp.concatenate(tiles, axis=1)


def down_matrix(held, piece, hid):
    tiles = [
        held[:, :, i * piece : (i + 1) * piece, :].reshape(-1, LANES)
        for i in range(2 * hid // LANES, 3 * hid // LANES)
    ]
    last = held[:, :, 3 * hid // LANES * piece :, :].reshape(SIDE * SIDE, piece // 2, LANES)
    last = jnp.concatenate([last[:, :, : LANES // 2], last[:, :, LANES // 2 :]], axis=1)
    return jnp.concatenate(tiles + [last.reshape(-1, LANES // 2)], axis=1)


def gated_product(both, hid):
    gate, up = both[:, :hid], both[:, hid:]
    return (gate / (1.0 + jnp.exp(-gate)) * up).astype(jnp.bfloat16)


def down_product(hidden, down):
    return lax.dot_general(hidden, down, (((1,), (1,)), ((), ())), preferred_element_type=jnp.float32)


def first_kernel(core_ref, rows_ref, weights_ref, out_ref, held, total, sems, *, piece, hid):
    per = 2
    span = per * SIDE * piece
    down_at = 2 * hid // LANES * piece
    core = core_ref[0]

    def copy(i, swapped, part):
        lines = (pl.ds(0, down_at), pl.ds(down_at, held.shape[2] - down_at))[part]
        source = weights_ref.at[:, i, lines] if swapped else weights_ref.at[i, :, lines]
        return pltpu.make_async_copy(source, held.at[i, :, lines], sems.at[part, i])

    for swapped in (False, True):

        @pl.when(core == int(swapped))
        def _():
            for part in range(2):
                for i in range(SIDE):
                    copy(i, swapped, part).start()

    both = None
    for step in range(SIDE // per):
        for i in range(step * per, (step + 1) * per):
            copy(i, False, 0).wait()
        part = jnp.dot(
            rows_ref[:, step * span : (step + 1) * span],
            gate_up(held, step * per, per, piece, hid),
            preferred_element_type=jnp.float32,
        )
        if step == 0:
            total[...] = part
        elif step < SIDE // per - 1:
            total[...] += part
        else:
            both = total[...] + part
    hidden = gated_product(both, hid)
    for i in range(SIDE):
        copy(i, False, 1).wait()
    out_ref[...] = down_product(hidden, down_matrix(held, piece, hid)).astype(out_ref.dtype)


def second_kernel(rows_ref, held, out_ref, *, piece, hid):
    both = jnp.dot(
        rows_ref[...], gate_up(held, 0, SIDE, piece, hid), preferred_element_type=jnp.float32
    )
    out_ref[...] = down_product(gated_product(both, hid), down_matrix(held, piece, hid)).astype(
        out_ref.dtype
    )


def ffn_cost(rows, width):
    count, depth = rows.shape
    return pl.CostEstimate(
        flops=2 * count * depth * width,
        bytes_accessed=2 * depth * width + 4 * rows.size,
        transcendentals=count * width // 3,
    )


def feed_forward_first(rows, weights, core, piece, width):
    count, depth = rows.shape
    vmem = pl.BlockSpec(memory_space=pltpu.VMEM)
    return pl.pallas_call(
        functools.partial(first_kernel, piece=piece, hid=width // 3),
        out_shape=(
            jax.ShapeDtypeStruct((count, depth), jnp.bfloat16),
            jax.ShapeDtypeStruct(weights.shape, weights.dtype),
        ),
        in_specs=[
            pl.BlockSpec(memory_space=pltpu.SMEM),
            vmem,
            pl.BlockSpec(memory_space=pl.ANY),
        ],
        out_specs=(vmem, vmem),
        scratch_shapes=[
            pltpu.VMEM((count, 2 * width // 3), jnp.float32),
            pltpu.SemaphoreType.DMA((2, SIDE)),
        ],
        cost_estimate=ffn_cost(rows, width),
        compiler_params=pltpu.CompilerParams(vmem_limit_bytes=FIRST_VMEM),
        name="ffn_first",
    )(core, rows, weights)


def feed_forward_second(rows, held, piece, width):
    vmem = pl.BlockSpec(memory_space=pltpu.VMEM)
    return pl.pallas_call(
        functools.partial(second_kernel, piece=piece, hid=width // 3),
        out_shape=jax.ShapeDtypeStruct(rows.shape, jnp.float32),
        in_specs=[vmem, vmem],
        out_specs=vmem,
        cost_estimate=ffn_cost(rows, width),
        compiler_params=pltpu.CompilerParams(vmem_limit_bytes=24 * 1024 * 1024),
        name="ffn_second",
    )(rows, held)


def halo_sides(block, axis, width):
    count = lax.axis_size(axis)
    forward = [(i, i + 1) for i in range(count - 1)]
    backward = [(target, source) for source, target in forward]
    low = lax.ppermute(block[:, -width:], axis, forward)
    high = lax.ppermute(block[:, :width], axis, backward)
    return low, high


def attend_block(query, band, valid, sink):
    heads = query.shape[1] // HEAD_DIM
    scaled = query * jnp.bfloat16(HEAD_DIM ** (-0.5))
    stacked = jnp.concatenate(
        [scaled[:, head * HEAD_DIM : (head + 1) * HEAD_DIM] for head in range(heads)], axis=0
    )
    scores = jnp.dot(stacked, band[:HEAD_DIM], preferred_element_type=jnp.float32)
    scores = jnp.where(jnp.concatenate([valid] * heads, axis=0), scores, -1e30)
    peak = jnp.maximum(jnp.max(scores, axis=1, keepdims=True), sink)
    raw = jnp.exp(scores - peak)
    denom = jnp.sum(raw, axis=1, keepdims=True) + jnp.exp(sink - peak)
    probs = (raw * (1.0 / denom)).astype(jnp.bfloat16)
    mixed = lax.dot_general(
        probs, band[HEAD_DIM:], (((1,), (1,)), ((), ())), preferred_element_type=jnp.float32
    ).astype(jnp.bfloat16)
    return jnp.concatenate(
        [mixed[head * WINDOW : (head + 1) * WINDOW] for head in range(heads)], axis=1
    )


def near_and_position():
    query_at = lax.broadcasted_iota(jnp.int32, (WINDOW, 3 * WINDOW), 0)
    key_at = lax.broadcasted_iota(jnp.int32, (WINDOW, 3 * WINDOW), 1)
    return (key_at >= query_at) & (key_at <= query_at + 2 * WINDOW), key_at


def sink_column(sink_ref, heads):
    return jnp.concatenate(
        [jnp.full((WINDOW, 1), sink_ref[head], jnp.float32) for head in range(heads)], axis=0
    )


def inner_kernel(sink_ref, query_ref, mid_ref, out_ref):
    near, _ = near_and_position()
    sink = sink_column(sink_ref, query_ref.shape[1] // HEAD_DIM)
    for at in range(WINDOW, query_ref.shape[0] - WINDOW, WINDOW):
        out_ref[at - WINDOW : at, :] = attend_block(
            query_ref[at : at + WINDOW, :], mid_ref[:, at - WINDOW : at + 2 * WINDOW], near, sink
        )


def attend_inner(queries, middle, sink_logit):
    rows, columns = queries.shape
    vmem = pl.BlockSpec(memory_space=pltpu.VMEM)
    return pl.pallas_call(
        inner_kernel,
        out_shape=jax.ShapeDtypeStruct((rows - 2 * WINDOW, columns), queries.dtype),
        in_specs=[pl.BlockSpec(memory_space=pltpu.SMEM), vmem, vmem],
        out_specs=vmem,
        cost_estimate=pl.CostEstimate(
            flops=12 * WINDOW * rows * columns,
            bytes_accessed=4 * rows * columns,
            transcendentals=WINDOW * rows * columns // HEAD_DIM,
        ),
        compiler_params=pltpu.CompilerParams(vmem_limit_bytes=16 * 1024 * 1024),
        name="inner",
    )(sink_logit, queries, middle)


def attention_kernel(
    place_ref, sink_ref, query_ref, low_ref, mid_ref, high_ref, inner_ref, proj_ref, mate_ref, mine_ref, attended
):
    rows = query_ref.shape[0]
    piece = WINDOW // CORES
    core, start, total = place_ref[0], place_ref[1], place_ref[2]
    near, key_at = near_and_position()
    sink = sink_column(sink_ref, query_ref.shape[1] // HEAD_DIM)
    first = jnp.concatenate([low_ref[...], mid_ref[:, : 2 * WINDOW]], axis=1)
    last = jnp.concatenate([mid_ref[:, rows - 2 * WINDOW :], high_ref[...]], axis=1)
    for at, band in ((0, first), (rows - WINDOW, last)):
        position = key_at + (start + at - WINDOW)
        valid = near & (position >= 0) & (position < total)
        attended[at : at + WINDOW, :] = attend_block(
            query_ref[at : at + WINDOW, :], band, valid, sink
        )
    attended[WINDOW : rows - WINDOW, :] = inner_ref[...]
    def picked(which):
        return jnp.concatenate(
            [
                attended[pl.ds(pl.multiple_of(at + which * piece, piece), piece), :]
                for at in range(0, rows, WINDOW)
            ],
            axis=0,
        )

    mine_ref[...] = picked(core)
    mate_ref[...] = jnp.dot(
        picked(1 - core), proj_ref[...], preferred_element_type=jnp.float32
    ).astype(mate_ref.dtype)


def attend_and_project(queries, sides, middle, inner, sink_logit, out_weight, place):
    rows, columns = queries.shape
    depth = out_weight.shape[1]
    low, high = sides
    vmem = pl.BlockSpec(memory_space=pltpu.VMEM)
    smem = pl.BlockSpec(memory_space=pltpu.SMEM)
    half = rows // CORES
    return pl.pallas_call(
        attention_kernel,
        out_shape=(
            jax.ShapeDtypeStruct((half, depth), jnp.bfloat16),
            jax.ShapeDtypeStruct((half, columns), jnp.bfloat16),
        ),
        in_specs=[smem, smem] + [vmem] * 6,
        out_specs=(vmem, vmem),
        scratch_shapes=[pltpu.VMEM((rows, columns), jnp.bfloat16)],
        cost_estimate=pl.CostEstimate(
            flops=2 * rows * columns * (6 * WINDOW + depth),
            bytes_accessed=8 * half * depth,
            transcendentals=3 * WINDOW * rows * columns // HEAD_DIM,
        ),
        compiler_params=pltpu.CompilerParams(vmem_limit_bytes=16 * 1024 * 1024),
        name="attend",
    )(place, sink_logit, queries, low, middle, high, inner, out_weight)


def norm_kernel(pieces_ref, residual_ref, gain_ref, mixed_ref, spread_ref):
    mixed = residual_ref[...].astype(jnp.float32)
    mixed += jnp.sum(pieces_ref[...].astype(jnp.float32), axis=0)
    mixed_ref[...] = mixed
    inverse = lax.rsqrt(jnp.mean(mixed * mixed, axis=1, keepdims=True) + 1e-06)
    normed = (mixed * inverse * gain_ref[...]).astype(spread_ref.dtype)
    for i in range(spread_ref.shape[0]):
        spread_ref[i] = normed


def sum_and_norm(pieces, residual, norm_gain):
    vmem = pl.BlockSpec(memory_space=pltpu.VMEM)
    return pl.pallas_call(
        norm_kernel,
        out_shape=(
            jax.ShapeDtypeStruct(residual.shape, jnp.float32),
            jax.ShapeDtypeStruct(pieces.shape, residual.dtype),
        ),
        in_specs=[vmem] * 3,
        out_specs=(vmem, vmem),
        compiler_params=pltpu.CompilerParams(vmem_limit_bytes=8 * 1024 * 1024),
        name="norm",
    )(pieces, residual, norm_gain.reshape(1, -1))


def last_kernel(pieces_ref, mixed_ref, out_ref):
    total = mixed_ref[...] + jnp.sum(pieces_ref[...].astype(jnp.float32), axis=0)
    out_ref[...] = total.astype(out_ref.dtype)


def last_sum(pieces, mixed):
    vmem = pl.BlockSpec(memory_space=pltpu.VMEM)
    return pl.pallas_call(
        last_kernel,
        out_shape=jax.ShapeDtypeStruct(mixed.shape, pieces.dtype),
        in_specs=[vmem] * 2,
        out_specs=vmem,
        compiler_params=pltpu.CompilerParams(vmem_limit_bytes=8 * 1024 * 1024),
        name="last",
    )(pieces, mixed)


def shards(
    queries,
    key_rows,
    values,
    sink_logit,
    residual_in,
    out_weight,
    norm_gain,
    gate_weight,
    up_weight,
    down_weight,
):
    rows_here, depth = queries.shape[0], residual_in.shape[1]
    sps, tps = lax.axis_size("sp"), lax.axis_size("tp")
    xs = tps // CORES
    own = rows_here // tps
    core = lax.axis_index("tp") % CORES
    both_axes = ("sp", "tp")

    mine = jnp.concatenate([gate_weight, up_weight, down_weight.T], axis=1)
    line = lax.all_to_all(
        pack_copies(mine),
        both_axes,
        0,
        0,
        tiled=True,
        axis_index_groups=line_groups(sps, tps, True),
    )
    line, queries, key_rows, values = lax.optimization_barrier((line, queries, key_rows, values))
    weights = lax.all_gather(
        line, both_axes, axis=0, tiled=False, axis_index_groups=line_groups(sps, tps, False)
    )

    middle = jnp.concatenate([key_rows.T, values.T], axis=0)
    sides = halo_sides(middle, "sp", WINDOW)
    place = jnp.stack([core, lax.axis_index("sp") * rows_here, jnp.int32(rows_here * sps)]).astype(
        jnp.int32
    )

    def swap(array):
        return lax.ppermute(array, "tp", core_swap(tps))

    def exchange(blocks):
        return lax.all_to_all(
            blocks.reshape(xs, own, depth), "tp", 0, 0, tiled=True, axis_index_groups=x_groups(tps)
        )

    def added(mine, mates):
        return exchange((mine + mates.astype(jnp.float32)).astype(jnp.bfloat16))

    mate_part, my_heads = attend_and_project(
        queries, sides, middle, attend_inner(queries, middle, sink_logit), sink_logit, out_weight, place
    )
    my_part = jnp.dot(my_heads, out_weight, preferred_element_type=jnp.float32)
    mixed_rows, spread = sum_and_norm(added(my_part, swap(mate_part)), residual_in, norm_gain)
    my_rows = exchange(spread).reshape(xs * own, depth)
    mate_rows = swap(my_rows)
    mate_out, held = feed_forward_first(
        mate_rows, weights, core.astype(jnp.int32).reshape(1), *mine.shape
    )
    mate_sum = swap(mate_out)
    my_out = feed_forward_second(my_rows, held, *mine.shape)
    return last_sum(added(my_out, mate_sum), mixed_rows)


def solution(mesh):
    return jax.shard_map(
        shards,
        mesh=mesh,
        in_specs=(
            P("sp", "tp"),
            P("sp", "tp"),
            P("sp", "tp"),
            P("tp"),
            P(("sp", "tp"), None),
            P("tp", None),
            P(),
            P("sp", "tp"),
            P("sp", "tp"),
            P("tp", "sp"),
        ),
        out_specs=P(("sp", "tp"), None),
        check_vma=False,
    )
```
